32 devices in a mesh: sp: 4 (over y, x), tp: 8 (over z, core).
Axes of the slice: x: 2, y: 2, z: 4, core: 2. Of those that a mesh axis runs over, the one named last changes fastest.
Arguments:
- lru_input: bfloat16 [1024, 2048], P('sp', 'tp'), may hold values from -27 to 27
- gate_input: bfloat16 [1024, 2048], P('sp', 'tp'), may hold values from -6 to 6
- documents: int32 [1024], P('sp'), may hold values from 0 to 1, never falling along the last dimension, each value on 1 to 768 neighbouring positions
- conv_taps: bfloat16 [4, 2048], P(None, 'tp'), may hold values from -3 to 3
- rate_weight: bfloat16 [16, 128, 128], P('tp'), may hold values from -0.5 to 0.5
- inlet_weight: bfloat16 [16, 128, 128], P('tp'), may hold values from -0.5 to 0.5
- decay_param: float32 [2048], P('tp')
- lru_gain: float32 [2048], P('tp'), may hold values from 0.1 to 1.9
- out_weight: bfloat16 [2048, 2048], P('tp'), may hold values from -0.125 to 0.125
- residual: bfloat16 [1024, 2048], P('sp'), may hold values from -6 to 6
- ffn_gain: float32 [2048], replicated, may hold values from 0.1 to 1.9
- routes: int32 [1024, 2], P('sp'), may hold values from 0 to 3, all different within a row; in each aligned block of 32 rows (0 to 31, 32 to 63, ...) at most 32 rows name the same one
- route_weights: float32 [1024, 2], P('sp'), may hold values from 0.1 to 0.9
- w_gate: bfloat16 [4, 2048, 6144], P('sp', None, 'tp'), may hold values from -0.125 to 0.125
- w_up: bfloat16 [4, 2048, 6144], P('sp', None, 'tp'), may hold values from -0.125 to 0.125
- w_down: bfloat16 [4, 6144, 2048], P('sp', 'tp'), may hold values from -0.078125 to 0.078125
Outputs:
- mixed_out: bfloat16 [1024, 2048], P(('sp', 'tp'))
The draws below stay inside these ranges and needn't reach their ends.
Inputs may be any that keep to these rules, and one draw needn't show every extreme that they name: `documents`: document numbers start at 0 and never fall along the sequence; a document spans at most 768 positions. `routes`: each row names 2 different experts. In each aligned block of 32 rows no expert is named by more than 32 rows, a bound that some block reaches.
All inputs are finite; a program needn't handle non-finite values.
Results may differ from the reference program's by a relative error of at most 0.017.
Values may be sent and summed in bfloat16 or wider, within the bound.
No kernel may reach another device: no remote copies, remote signals or barrier semaphores. Data moves between devices by JAX's collectives and lax.ppermute only.
A program may use at most 64 MiB of HBM per device.

```python
import math
import jax
import jax.numpy as jnp
import numpy as np
from jax import lax

D = 2048
D_RNN = 2048
LRU_BLOCKS = 16
LRU_BLOCK = 128
CONV_TAPS = 4
FF = 6144
TOP = 2
TOKENS = 1024
ROUTE_ROWS = 32
EXPERTS = 4
CAP = 32
DOCS = 2
DOC_MOST = 768
N_TP = 8


def draw_lru_input(key, part):
    base_key, group_key, span_key = jax.random.split(jax.random.fold_in(key, 11), 3)
    group_levels = jax.random.uniform(group_key, (LRU_BLOCKS,), jnp.float32, -1.2, 1.2)
    span_levels = jax.random.uniform(span_key, (TOKENS // 64,), jnp.float32, -0.7, 0.7)
    channel_scale = jnp.repeat(jnp.exp(group_levels), LRU_BLOCK)
    position_scale = jnp.repeat(jnp.exp(span_levels), 64)
    base_values = jnp.clip(jax.random.normal(base_key, (TOKENS, D_RNN), jnp.float32), -4.0, 4.0)
    return (base_values * channel_scale[None, :] * position_scale[:, None]).astype(jnp.bfloat16)


def draw_decay_param(key, part):
    pick_key, slow_key, fast_key = jax.random.split(jax.random.fold_in(key, 23), 3)
    slow_share = 0.5
    slow_pick = jax.random.uniform(pick_key, (D_RNN,), jnp.float32) < slow_share
    slow_value = math.log(2.5 * TOKENS) + jax.random.uniform(slow_key, (D_RNN,), jnp.float32, 0.0, 1.5)
    fast_value = jnp.log(jax.random.uniform(fast_key, (D_RNN,), jnp.float32, 120.0, 400.0))
    return jnp.where(slow_pick, slow_value, fast_value).astype(jnp.float32)


def block_levels(rng, extent, pieces, smallest, largest):
    level = 1.0
    for axis_at, parts in pieces:
        steps = jax.random.uniform(jax.random.fold_in(jax.random.fold_in(rng, 6), axis_at), (parts,), jnp.float32, smallest / len(pieces), largest / len(pieces))
        level = level * jnp.repeat(jnp.exp(steps), extent[axis_at] // parts).reshape((-1,) + (1,) * (len(extent) - 1 - axis_at))
    return level


def profile(number_of, total, reach, slope):
    weights = [(1 << 20) // math.isqrt(standing ** slope) + 1 for standing in range(2, number_of + 1)]
    surplus, counts = total - reach - (number_of - 1), [1] * (number_of - 1)
    while surplus > 0:
        movable = [i for i in range(number_of - 1) if counts[i] < reach]
        pool, budget = sum([weights[i] for i in movable]), surplus
        for i in movable:
            more = min(reach - counts[i], max(1, budget * weights[i] // pool), surplus)
            counts[i] = counts[i] + more
            surplus = surplus - more
    return np.array([reach] + counts)


def ragged_sizes(key, count, total, bound, lean):
    if count == 2:
        one = jax.random.randint(key, (), max(1, total - bound), min(bound, total - 1) + 1)
        return jnp.stack([one, total - one])
    lengths = jnp.asarray(profile(count, total, bound, lean), jnp.int32)
    twos = (count - 1) // 2
    donor, receiver = lengths[1:1 + 2 * twos:2], lengths[2:2 + 2 * twos:2]
    slack = jnp.minimum(donor - 1, bound - receiver)
    moved = jax.random.randint(jax.random.fold_in(key, 1), (twos,), 0, 1 << 20) % (slack + 1)
    lengths = lengths.at[1:1 + 2 * twos:2].set(donor - moved).at[2:2 + 2 * twos:2].set(receiver + moved)
    return lengths[jax.random.permutation(jax.random.fold_in(key, 2), count)]


def deal_out(key, own, number, rows, number_of, top, limit, lean):
    sequence = jax.random.permutation(key, number_of)
    packed, common = load_shares(number_of, rows * top, limit, lean, True), load_shares(number_of, rows * top, limit, lean, False)
    places = jnp.arange(number_of)

    def named(tallies, rotation):
        used = int((tallies > 0).sum())
        fixed = max(1, used // 4)
        passed = fixed + (places - fixed + rotation * (used - fixed)) % max(1, number_of - fixed)
        return jnp.zeros((number_of,), jnp.int32).at[sequence[jnp.where(places < fixed, places, passed)]].set(jnp.asarray(tallies, jnp.int32))

    tallies = jnp.where(number % 4 == 0, named(packed, number // 4), named(common, number - number // 4 - 1))
    mixed = jax.random.permutation(jax.random.fold_in(own, 3), number_of)
    donor, sink = mixed[0:number_of // 2 * 2:2], mixed[1:number_of // 2 * 2:2]
    room = jnp.minimum(tallies[donor] - 1, limit - tallies[sink]) // 2
    room = jnp.where((donor == sequence[0]) | (sink == sequence[0]) | (tallies[sink] == 0), 0, jnp.maximum(room, 0))
    passed = jax.random.randint(jax.random.fold_in(own, 4), (number_of // 2,), 0, 1 << 20) % (room + 1)
    tallies = tallies.at[donor].add(-passed).at[sink].add(passed)
    members = jnp.searchsorted(jnp.cumsum(tallies), jnp.arange(rows * top), side="right").astype(jnp.int32)
    listing = members.reshape(top, rows).T
    listing = listing[jax.random.permutation(jax.random.fold_in(own, 1), rows)]
    rotation = jax.random.randint(jax.random.fold_in(own, 2), (rows, 1), 0, top)
    return jnp.take_along_axis(listing, (jnp.arange(top)[None, :] + rotation) % top, axis=1)


def load_shares(number_of, total, reach, slope, full):
    weights = [(1 << 20) // math.isqrt(grade ** slope) + 1 for grade in range(1, number_of + 1)]
    largest = reach if full else min(reach, max(-(-total // number_of), total * weights[0] // sum(weights)))
    least = 1 if total - largest >= number_of - 1 else 0
    given, rest = [largest] + [least] * (number_of - 1), total - largest - least * (number_of - 1)
    while rest > 0:
        movable = [i for i in range(1, number_of) if given[i] < largest] or [i for i in range(1, number_of) if given[i] < reach]
        whole, left = sum([weights[i] for i in movable]), rest
        for i in movable:
            more = min(reach - given[i], max(1, left * weights[i] // whole), rest)
            given[i] = given[i] + more
            rest = rest - more
    return np.array(given)


def normal_values(stream_key, dims, deviation, limit, cuts=(), kind=jnp.bfloat16):
    values = deviation * jax.random.normal(stream_key, dims, jnp.float32)
    if cuts:
        values = values * block_levels(stream_key, dims, cuts, -0.22, 0.18)
    return jnp.clip(values, -limit, limit).astype(kind)


def setup_inputs(seed: int = 0) -> dict:
    arg_keys = jax.random.split(jax.random.key(seed), 17)
    lru_input = draw_lru_input(jax.random.fold_in(arg_keys[16], 71), 0)
    gate_input = normal_values(arg_keys[1], (TOKENS, D_RNN), 1.0, 6.0, ((0, 4), (1, 8)))
    documents = jnp.searchsorted(jnp.cumsum(ragged_sizes(arg_keys[2], DOCS, TOKENS, DOC_MOST, 0)), jnp.arange(TOKENS), side="right").astype(jnp.int32)
    conv_taps = normal_values(arg_keys[3], (CONV_TAPS, D_RNN), CONV_TAPS ** -0.5, 3.0, ((1, 8),))
    rate_weight = normal_values(arg_keys[4], (LRU_BLOCKS, LRU_BLOCK, LRU_BLOCK), LRU_BLOCK ** -0.5, 0.5, ((0, 8),))
    inlet_weight = normal_values(arg_keys[5], (LRU_BLOCKS, LRU_BLOCK, LRU_BLOCK), LRU_BLOCK ** -0.5, 0.5, ((0, 8),))
    decay_param = draw_decay_param(jax.random.fold_in(arg_keys[16], 71), 0)
    lru_gain = jnp.clip(1.0 + 0.18 * jax.random.normal(arg_keys[7], (D_RNN,), jnp.float32), 0.1, 1.9)
    out_weight = normal_values(arg_keys[8], (D_RNN, D), D_RNN ** -0.5, 0.125, ((0, 8),))
    residual = normal_values(arg_keys[9], (TOKENS, D), 1.0, 6.0, ((0, 4),))
    ffn_gain = jnp.clip(1.0 + 0.18 * jax.random.normal(arg_keys[10], (D,), jnp.float32), 0.1, 1.9)
    routes_keys = jax.random.split(jax.random.fold_in(arg_keys[11], 1), TOKENS // ROUTE_ROWS)
    routes_turns = jax.random.permutation(jax.random.fold_in(arg_keys[11], 3), TOKENS // ROUTE_ROWS)
    routes = jax.vmap(lambda own, number: deal_out(jax.random.fold_in(arg_keys[11], 2), own, number, ROUTE_ROWS, EXPERTS, TOP, CAP, 2))(routes_keys, routes_turns).reshape((TOKENS, TOP))
    route_weights = jnp.clip(0.1 + 0.79999997 * jax.random.uniform(arg_keys[12], (TOKENS, TOP), jnp.float32) ** block_levels(arg_keys[12], (TOKENS, TOP), ((0, 4),), -0.2, 0.2), 0.1, 0.9)
    w_gate = normal_values(arg_keys[13], (EXPERTS, D, FF), D ** -0.5, 0.125, ((0, 4), (2, 8)))
    w_up = normal_values(arg_keys[14], (EXPERTS, D, FF), D ** -0.5, 0.125, ((0, 4), (2, 8)))
    w_down = normal_values(arg_keys[15], (EXPERTS, FF, D), FF ** -0.5, 0.078125, ((0, 4), (1, 8)))
    return {"lru_input": lru_input, "gate_input": gate_input, "documents": documents, "conv_taps": conv_taps, "rate_weight": rate_weight, "inlet_weight": inlet_weight, "decay_param": decay_param, "lru_gain": lru_gain, "out_weight": out_weight, "residual": residual, "ffn_gain": ffn_gain, "routes": routes, "route_weights": route_weights, "w_gate": w_gate, "w_up": w_up, "w_down": w_down}


EPSILON = 1e-06
RATE_SCALE = 8.0

def join_runs(earlier_run, later_run):
    return (earlier_run[0] * later_run[0], later_run[0] * earlier_run[1] + later_run[1])

def slot_targets(route_block, expert_count, capacity):
    flat_routes = route_block.reshape(-1)
    onehot = (flat_routes[:, None] == jnp.arange(expert_count, dtype=jnp.int32)[None, :]).astype(jnp.int32)
    earlier_hits = jnp.cumsum(onehot, axis=0) - onehot
    slot_index = lax.optimization_barrier(jnp.sum(earlier_hits * onehot, axis=1))
    return (flat_routes * capacity + slot_index).astype(jnp.int32).reshape(route_block.shape)

def rms_rows(row_block, gain_vector):
    floated = row_block.astype(jnp.float32)
    inverse_rms = lax.rsqrt(lax.optimization_barrier(jnp.mean(floated * floated, axis=1, keepdims=True)) + EPSILON)
    return (floated * inverse_rms * gain_vector.astype(jnp.float32)[None, :]).astype(jnp.bfloat16)

def summed_blocks(left_rows, right_rows, blocks):
    span_width = left_rows.shape[1] // blocks

    def add_block(running, block_index):
        start_col = (block_index * span_width).astype(jnp.int32)
        partial_sum = jnp.dot(lax.dynamic_slice_in_dim(left_rows, start_col, span_width, 1), lax.dynamic_slice_in_dim(right_rows, start_col, span_width, 0), preferred_element_type=jnp.float32)
        partial_sum = lax.optimization_barrier(partial_sum.astype(jnp.bfloat16)).astype(jnp.float32)
        return (running + partial_sum, None)
    running, _ = lax.scan(add_block, jnp.zeros((left_rows.shape[0], right_rows.shape[1]), jnp.float32), jnp.arange(blocks, dtype=jnp.int32))
    return running

def reference(lru_input, gate_input, documents, conv_taps, rate_weight, inlet_weight, decay_param, lru_gain, out_weight, residual, ffn_gain, routes, route_weights, w_gate, w_up, w_down):
    documents = documents.astype(jnp.int32)
    reach_back = CONV_TAPS - 1
    prior_docs = jnp.concatenate([jnp.full((reach_back,), -1, jnp.int32), documents])
    padded_input = jnp.concatenate([jnp.zeros((reach_back, D_RNN), jnp.bfloat16), lru_input], axis=0)
    conv_sum = jnp.zeros((TOKENS, D_RNN), jnp.float32)
    for tap_index in range(CONV_TAPS):
        same_doc = (prior_docs[tap_index:tap_index + TOKENS] == documents).astype(jnp.float32)[:, None]
        conv_sum = conv_sum + padded_input[tap_index:tap_index + TOKENS].astype(jnp.float32) * conv_taps[tap_index].astype(jnp.float32)[None, :] * same_doc
    convolved = conv_sum.astype(jnp.bfloat16)
    grouped = convolved.astype(jnp.float32).reshape(TOKENS, LRU_BLOCKS, LRU_BLOCK)
    rate_gate = jax.nn.sigmoid(jnp.einsum('tnc,ncd->tnd', grouped, rate_weight.astype(jnp.float32)).reshape(TOKENS, D_RNN))
    inlet_gate = jax.nn.sigmoid(jnp.einsum('tnc,ncd->tnd', grouped, inlet_weight.astype(jnp.float32)).reshape(TOKENS, D_RNN))
    log_decay = -RATE_SCALE * rate_gate * jax.nn.softplus(-decay_param.astype(jnp.float32))[None, :]
    starts = (prior_docs[reach_back - 1:reach_back - 1 + TOKENS] != documents)[:, None]
    decay_step = jnp.where(starts, 0.0, jnp.exp(log_decay))
    norm_factor = jnp.where(starts, 1.0, jnp.sqrt(-jnp.expm1(2.0 * log_decay)))
    drive_term = norm_factor * inlet_gate * convolved.astype(jnp.float32)
    _, hidden_state = lax.associative_scan(join_runs, (decay_step, drive_term), axis=0)
    inverse_rms = lax.rsqrt(lax.optimization_barrier(jnp.mean(hidden_state * hidden_state, axis=1, keepdims=True)) + EPSILON)
    mixer_rows = (hidden_state * inverse_rms * lru_gain.astype(jnp.float32)[None, :] * jax.nn.gelu(gate_input.astype(jnp.float32))).astype(jnp.bfloat16)
    projected = summed_blocks(mixer_rows, out_weight, N_TP)
    after_mixer = (residual.astype(jnp.float32) + projected).astype(jnp.bfloat16)
    normed = rms_rows(after_mixer, ffn_gain)
    block_count = TOKENS // ROUTE_ROWS
    route_blocks = routes.astype(jnp.int32).reshape(block_count, ROUTE_ROWS, TOP)

    def block_slots(route_block):
        return slot_targets(route_block, EXPERTS, CAP)
    targets = jax.vmap(block_slots)(route_blocks)
    slot_index = targets - route_blocks * CAP
    block_ids = jnp.arange(block_count, dtype=jnp.int32)[:, None, None]
    buffer_rows = ((route_blocks * block_count + block_ids) * CAP + slot_index).astype(jnp.int32).reshape(-1)
    token_ids = jnp.broadcast_to(jnp.arange(TOKENS, dtype=jnp.int32).reshape(block_count, ROUTE_ROWS, 1), route_blocks.shape).reshape(-1)
    slot_table = jnp.zeros((EXPERTS * block_count * CAP,), jnp.int32).at[buffer_rows].set(token_ids + 1)
    padded_normed = jnp.concatenate([jnp.zeros((1, D), jnp.bfloat16), normed], axis=0)
    expert_span = block_count * CAP

    def run_expert(expert_id):
        picked_ids = lax.dynamic_slice_in_dim(slot_table, (expert_id * expert_span).astype(jnp.int32), expert_span, 0)
        expert_in = padded_normed[picked_ids]
        gate_part = jnp.dot(expert_in, w_gate[expert_id], preferred_element_type=jnp.float32)
        up_part = jnp.dot(expert_in, w_up[expert_id], preferred_element_type=jnp.float32)
        hidden_units = (jax.nn.silu(gate_part) * up_part).astype(jnp.bfloat16)
        return summed_blocks(hidden_units, w_down[expert_id], N_TP).astype(jnp.bfloat16)
    expert_out = lax.map(run_expert, jnp.arange(EXPERTS, dtype=jnp.int32))
    gathered = expert_out.reshape(EXPERTS * expert_span, D)[buffer_rows].astype(jnp.float32).reshape(TOKENS, TOP, D)
    routed = lax.optimization_barrier(jnp.sum(gathered * route_weights.astype(jnp.float32)[:, :, None], axis=1))
    return (after_mixer.astype(jnp.float32) + routed).astype(jnp.bfloat16)
```

```python
import functools

import jax
import jax.numpy as jnp
from jax import lax
from jax.experimental import pallas as pl
from jax.experimental.pallas import tpu as pltpu
from jax.sharding import PartitionSpec as P

EPSILON = 1e-06
RATE_SCALE = 8.0
LANES = 128
SUBLANES = 8
CORES = 2
PLANE = 4


F32 = jnp.float32
BF16 = jnp.bfloat16
SMEM = pl.BlockSpec(memory_space=pltpu.SMEM)


def flip(value, axis, distance):
    return lax.ppermute(value, axis, [(i, i ^ distance) for i in range(lax.axis_size(axis))])


def flip_z(value, distance):
    return flip(value, "tp", distance * CORES)


def column(row):
    return jnp.transpose(jnp.broadcast_to(row, (LANES, row.shape[1])))


def one_minus_exp(value):
    series = jnp.ones_like(value)
    for order in range(7, 1, -1):
        series = 1.0 + value * series * (1.0 / order)
    return jnp.where(value > -0.35, -value * series, 1.0 - jnp.exp(value))


def scan_rows(decay, drive):
    rows = decay.shape[0]
    row_ids = lax.broadcasted_iota(jnp.int32, decay.shape, 0)
    distance = 1
    while distance < rows:
        if distance < SUBLANES:
            head = row_ids < distance
            earlier_decay = jnp.where(head, 1.0, pltpu.roll(decay, distance, 0))
            earlier_drive = jnp.where(head, 0.0, pltpu.roll(drive, distance, 0))
            drive = drive + decay * earlier_drive
            decay = decay * earlier_decay
        else:
            late_drive = drive[distance:] + decay[distance:] * drive[: rows - distance]
            late_decay = decay[distance:] * decay[: rows - distance]
            drive = jnp.concatenate([drive[:distance], late_drive], axis=0)
            decay = jnp.concatenate([decay[:distance], late_decay], axis=0)
        distance *= 2
    return decay, drive


def lru_kernel(
    here, rows_in, gate_in, tail, docs, taps, rate_w, inlet_w, decay_in, gain, routes, route_w,
    state_out, run_out, mix_out, *rest,
):
    *messages, padded, doc_cols = rest
    positions, channels = rows_in.shape
    reach = taps.shape[0] - 1
    first = SUBLANES - reach
    padded[0:SUBLANES] = tail[0:SUBLANES]
    padded[SUBLANES:] = rows_in[...].astype(F32)
    doc_cols[0:SUBLANES] = column(tail[SUBLANES : SUBLANES + 1, 0:LANES])[LANES - SUBLANES :]
    doc_cols[SUBLANES:] = column(docs[...].astype(F32) + 1.0)
    own_doc = doc_cols[SUBLANES:]
    starts = doc_cols[SUBLANES - 1 : SUBLANES - 1 + positions] != own_doc
    for group in range(channels // LANES):
        lanes = slice(group * LANES, (group + 1) * LANES)
        conv = jnp.zeros((positions, LANES), F32)
        for tap in range(reach + 1):
            shifted_rows = padded[first + tap : first + tap + positions, lanes]
            if tap < reach:
                same = doc_cols[first + tap : first + tap + positions] == own_doc
                shifted_rows = jnp.where(same, shifted_rows, 0.0)
            conv = conv + shifted_rows * taps[tap : tap + 1, lanes].astype(F32)
        conv = conv.astype(BF16)
        rate = jax.nn.sigmoid(jnp.dot(conv, rate_w[group], preferred_element_type=F32))
        inlet = jax.nn.sigmoid(jnp.dot(conv, inlet_w[group], preferred_element_type=F32))
        negated = -decay_in[0:1, lanes]
        soft = jnp.maximum(negated, 0.0) + jnp.log1p(jnp.exp(-jnp.abs(negated)))
        log_decay = -RATE_SCALE * rate * soft
        decay = jnp.where(starts, 0.0, jnp.exp(log_decay))
        norm = jnp.where(starts, 1.0, jnp.sqrt(one_minus_exp(2.0 * log_decay)))
        run, state = scan_rows(decay, norm * inlet * conv.astype(F32))
        state_out[:, lanes] = state
        run_out[:, lanes] = run
        mix_out[:, lanes] = jax.nn.gelu(gate_in[:, lanes].astype(F32)) * gain[0:1, lanes]
        for message in messages:
            message[0:1, lanes] = run[positions - 1 :]
            message[1:2, lanes] = state[positions - 1 :]
    shard = here[0]
    lane_ids = lax.broadcasted_iota(jnp.int32, (positions, LANES), 1)
    dense = jnp.zeros((positions, LANES), F32)
    for choice in range(routes.shape[1]):
        relative = routes[:, choice : choice + 1] ^ shard
        dense = dense + jnp.where(relative == lane_ids, route_w[:, choice : choice + 1], 0.0)
    dense = jnp.transpose(dense)
    for k, message in enumerate(messages):
        message[2:3, 0:positions] = dense[k : k + 1]


def split_sum(total):
    lane_ids = lax.broadcasted_iota(jnp.int32, (total.shape[0], LANES), 1)
    high = total.astype(BF16).astype(F32)
    low = (total - high).astype(BF16).astype(F32)
    return jnp.where(lane_ids == 0, high, jnp.where(lane_ids == 1, low, 0.0)).astype(BF16)


def joined_sum(lanes):
    lanes = lanes.astype(F32)
    return lanes[:, 0:1] + lanes[:, 1:2]


def mix_kernel(here, state, run, mix, *rest, block):
    *messages, keep, send, stacked, mixed = rest
    channels = state.shape[1]
    for k, message in enumerate(messages):
        stacked[k] = message[...]
    shard, core = here[0], here[2]

    def hop(position, carried):
        run_state = stacked[position ^ shard]
        return run_state[0:1, :channels] * carried + run_state[1:2, :channels]

    carried = lax.fori_loop(0, shard, hop, jnp.zeros((1, channels), F32))
    hidden = state[...] + run[...] * carried
    mixed[:, :channels] = (hidden * mix[...]).astype(BF16)
    mixed[:, channels:] = split_sum(jnp.sum(hidden * hidden, axis=1, keepdims=True))
    for z in range(keep.shape[0] // block):
        rows = slice(z * block, (z + 1) * block)
        keep[rows] = mixed[pl.ds(pl.multiple_of((CORES * z + core) * block, block), block)]
        send[rows] = mixed[pl.ds(pl.multiple_of((CORES * z + 1 - core) * block, block), block)]


def project_kernel(here, keep, other, own_w, other_w, *rest, block):
    *outs, own_rows, other_rows = rest
    channels, width = own_w.shape
    depth = here[1]
    for k in range(len(outs)):
        rows = slice(k * block, (k + 1) * block)
        source = pl.ds(pl.multiple_of((depth ^ k) * block, block), block)
        own_rows[rows] = keep[source]
        other_rows[rows] = other[source]
    squares = split_sum(joined_sum(own_rows[:, channels:]) + joined_sum(other_rows[:, channels:]))
    product = jnp.dot(own_rows[:, :channels], own_w[...], preferred_element_type=F32)
    product = product + jnp.dot(other_rows[:, :channels], other_w[...], preferred_element_type=F32)
    for k, out in enumerate(outs):
        rows = slice(k * block, (k + 1) * block)
        out[:, :width] = product[rows].astype(BF16)
        out[:, width:] = squares[rows]


def norm_kernel(here, residual, gain, *rest, channels_total):
    *parts, after_out, normed_out = rest
    width = residual.shape[1]
    total = sum(part[:, :width].astype(F32) for part in parts)
    squares = sum(joined_sum(part[:, width:]) for part in parts)
    projected = total * lax.rsqrt(squares / channels_total + EPSILON)
    after = (residual[...].astype(F32) + projected).astype(BF16)
    after_out[...] = after
    floated = after.astype(F32)
    inverse_rms = lax.rsqrt(jnp.mean(floated * floated, axis=1, keepdims=True) + EPSILON)
    normed_out[...] = (floated * inverse_rms * gain[...]).astype(BF16)


def expert_kernel(here, *refs, labels, block, tiles):
    pieces, refs = refs[: len(labels)], refs[len(labels) :]
    messages, refs = refs[:PLANE], refs[PLANE:]
    (own_gate, other_gate, own_up, other_up, own_down, other_down), refs = refs[:6], refs[6:]
    outs, (tokens, weight_cols, weights, hidden) = refs[: len(labels)], refs[len(labels) :]
    step = pl.program_id(0)
    tile = own_gate.shape[1]
    half = own_down.shape[0]

    @pl.when(step == 0)
    def _():
        positions = weight_cols.shape[1]
        for k in range(PLANE):
            weight_cols[k] = column(messages[k][2:3, :positions])
        at = 0
        for piece, (z_flip, planes) in zip(pieces, labels):
            tokens[at : at + len(planes) * block] = piece[...]
            source = (CORES * (here[1] ^ z_flip) + here[2]) * block
            for k in planes:
                weights[at : at + block] = weight_cols[k, pl.ds(pl.multiple_of(source, block), block)]
                at += block

    def hide(gate_w, up_w, at):
        rows = tokens[...]
        gate = jnp.dot(rows, gate_w[...], preferred_element_type=F32)
        up = jnp.dot(rows, up_w[...], preferred_element_type=F32)
        hidden[:, at : at + tile] = (jax.nn.silu(gate) * up).astype(BF16)

    for index in range(2 * tiles):
        if index < tiles:
            arm = functools.partial(hide, own_gate, own_up, index * tile)
        else:
            arm = functools.partial(hide, other_gate, other_up, index * tile)
        pl.when(step == index)(arm)

    @pl.when(step >= 2 * tiles)
    def _():
        product = jnp.dot(hidden[:, :half], own_down[...], preferred_element_type=F32)
        product = product + jnp.dot(hidden[:, half:], other_down[...], preferred_element_type=F32)
        scaled = jnp.concatenate(
            [
                product[:, at : at + LANES] * weights[...]
                for at in range(0, product.shape[1], LANES)
            ],
            axis=1,
        ).astype(BF16)
        at = 0
        for out in outs:
            out[...] = scaled[at : at + out.shape[0]]
            at += out.shape[0]


def run_experts(here, pieces, labels, messages, weights, block):
    own_gate, other_gate, own_up, other_up, own_down, other_down = weights
    width, half = own_gate.shape
    tile, out_tile = 2 * LANES, 4 * LANES
    tiles, out_tiles = half // tile, width // out_tile
    rows = sum(piece.shape[0] for piece in pieces)
    positions = block * lax.axis_size("tp")

    def whole(value):
        return pl.BlockSpec(value.shape, lambda i: (0, 0))

    def own_col(i):
        return (0, jnp.minimum(i, tiles - 1))

    def other_col(i):
        return (0, jnp.clip(i - tiles, 0, tiles - 1))

    def out_col(i):
        return (0, jnp.maximum(i - 2 * tiles, 0))

    return pl.pallas_call(
        functools.partial(expert_kernel, labels=labels, block=block, tiles=tiles),
        grid=(2 * tiles + out_tiles,),
        in_specs=[SMEM]
        + [whole(piece) for piece in pieces]
        + [whole(message) for message in messages]
        + [
            pl.BlockSpec((width, tile), own_col),
            pl.BlockSpec((width, tile), other_col),
            pl.BlockSpec((width, tile), own_col),
            pl.BlockSpec((width, tile), other_col),
            pl.BlockSpec((half, out_tile), out_col),
            pl.BlockSpec((half, out_tile), out_col),
        ],
        out_specs=[pl.BlockSpec((piece.shape[0], out_tile), out_col) for piece in pieces],
        out_shape=[jax.ShapeDtypeStruct(piece.shape, BF16) for piece in pieces],
        scratch_shapes=[
            pltpu.VMEM((rows, width), BF16),
            pltpu.VMEM((PLANE, positions, LANES), F32),
            pltpu.VMEM((rows, LANES), F32),
            pltpu.VMEM((rows, 2 * half), BF16),
        ],
    )(here, *pieces, *messages, *weights)


def fits(mesh, capacity_is_rows):
    return mesh["sp"] == PLANE and capacity_is_rows


def local_dense(
    lru_input, gate_input, documents, conv_taps, rate_weight, inlet_weight, decay_param, lru_gain,
    out_weight, residual, ffn_gain, routes, route_weights, w_gate, w_up, w_down,
):
    positions, channels = lru_input.shape
    width = residual.shape[1]
    tp_count = lax.axis_size("tp")
    depths = tp_count // CORES
    block = positions // tp_count
    tp_here = lax.axis_index("tp")
    here = jnp.stack(
        [lax.axis_index("sp"), tp_here // CORES, tp_here % CORES, tp_here]
    ).astype(jnp.int32)
    span = max(positions, channels)

    last_rows = lru_input[positions - SUBLANES :].astype(F32)
    last_docs = (documents[positions - LANES :] + 1).astype(F32)[None, :]
    last_docs = jnp.pad(last_docs, ((0, 0), (0, channels - LANES)))
    tail = lax.ppermute(
        jnp.concatenate([last_rows, last_docs], axis=0),
        "sp",
        [(i, i + 1) for i in range(PLANE - 1)],
    )
    swapped = [flip(value, "tp", 1) for value in (out_weight, w_gate[0], w_up[0], w_down[0])]

    state, run, mix, *messages = pl.pallas_call(
        lru_kernel,
        in_specs=[SMEM] + [pl.BlockSpec(memory_space=pltpu.VMEM)] * 11,
        out_shape=[jax.ShapeDtypeStruct((positions, channels), F32)] * 3
        + [jax.ShapeDtypeStruct((SUBLANES, span), F32)] * PLANE,
        scratch_shapes=[
            pltpu.VMEM((SUBLANES + positions, channels), F32),
            pltpu.VMEM((SUBLANES + positions, LANES), F32),
        ],
    )(
        here, lru_input, gate_input, tail, documents[None, :], conv_taps, rate_weight,
        inlet_weight, decay_param[None, :], lru_gain[None, :], routes, route_weights,
    )
    messages = [messages[0]] + [flip(messages[k], "sp", k) for k in range(1, PLANE)]

    half_rows = positions // CORES
    keep, send = pl.pallas_call(
        functools.partial(mix_kernel, block=block),
        in_specs=[SMEM] + [pl.BlockSpec(memory_space=pltpu.VMEM)] * (3 + PLANE),
        out_shape=[jax.ShapeDtypeStruct((half_rows, channels + LANES), BF16)] * 2,
        scratch_shapes=[
            pltpu.VMEM((PLANE, SUBLANES, span), F32),
            pltpu.VMEM((positions, channels + LANES), BF16),
        ],
    )(here, state, run, mix, *messages)
    other = flip(send, "tp", 1)

    parts = pl.pallas_call(
        functools.partial(project_kernel, block=block),
        in_specs=[SMEM] + [pl.BlockSpec(memory_space=pltpu.VMEM)] * 4,
        out_shape=[jax.ShapeDtypeStruct((block, width + LANES), BF16)] * depths,
        scratch_shapes=[pltpu.VMEM((half_rows, channels + LANES), BF16)] * 2,
    )(here, keep, other, out_weight, swapped[0])
    parts = [parts[0]] + [flip_z(parts[k], k) for k in range(1, depths)]

    after, normed = pl.pallas_call(
        functools.partial(norm_kernel, channels_total=channels * tp_count),
        grid_spec=pltpu.PrefetchScalarGridSpec(
            num_scalar_prefetch=1,
            grid=(1,),
            in_specs=[
                pl.BlockSpec((block, width), lambda i, at: (at[3], 0)),
                pl.BlockSpec((1, width), lambda i, at: (0, 0)),
            ]
            + [pl.BlockSpec((block, width + LANES), lambda i, at: (0, 0))] * depths,
            out_specs=[pl.BlockSpec((block, width), lambda i, at: (0, 0))] * 2,
        ),
        out_shape=[jax.ShapeDtypeStruct((block, width), BF16)] * 2,
    )(here, residual, ffn_gain[None, :], *parts)

    weights = (w_gate[0], swapped[1], w_up[0], swapped[2], w_down[0], swapped[3])
    rows_at = [normed] + [flip_z(normed, k) for k in range(1, depths)]
    finished = []
    for chunk in range(0, depths, 2):
        pieces, labels, orders = [], [], []
        for z_flip in range(chunk, min(chunk + 2, depths)):
            near, far = (1, 2) if z_flip % 2 == 0 else (2, 1)
            pair = jnp.concatenate([rows_at[z_flip], flip(rows_at[z_flip], "sp", near)], axis=0)
            pieces += [pair, flip(pair, "sp", far)]
            labels += [(z_flip, (0, near)), (z_flip, (far, 3))]
            orders.append((near, far))
        outs = run_experts(here, pieces, tuple(labels), messages, weights, block)
        for index, (near, far) in enumerate(orders):
            summed = outs[2 * index].astype(F32) + flip(outs[2 * index + 1], "sp", far).astype(F32)
            crossing = flip(summed[block:].astype(BF16), "sp", near)
            finished.append((summed[:block].astype(BF16).astype(F32) + crossing.astype(F32)).astype(BF16))
    total = after.astype(F32) + finished[0].astype(F32)
    for k in range(1, depths):
        total = total + flip_z(finished[k], k).astype(F32)
    return total.astype(BF16)


def shifted(block, axis, distance):
    devices = range(lax.axis_size(axis))
    route = [(i - distance, i) for i in devices if i - distance in devices]
    return lax.ppermute(block, axis, route)


def carried_in(value, axis, join, neutral):
    count, mine = (lax.axis_size(axis), lax.axis_index(axis))
    pieces = jax.tree.map(lambda part: lax.all_gather(part, axis), value)
    so_far = jax.tree.map(
        lambda part, zero: jnp.full_like(part, 0) + jnp.asarray(zero, part.dtype), value, neutral
    )

    def hop(position, so_far):
        longer = join(so_far, jax.tree.map(lambda part: part[position], pieces))
        return jax.tree.map(lambda new, old: jnp.where(position < mine, new, old), longer, so_far)

    return lax.fori_loop(0, count - 1, hop, so_far)


def join_runs(earlier_run, later_run):
    return (earlier_run[0] * later_run[0], later_run[0] * earlier_run[1] + later_run[1])


def slot_targets(route_block, expert_count, capacity):
    flat_routes = route_block.reshape(-1)
    onehot = (flat_routes[:, None] == jnp.arange(expert_count, dtype=jnp.int32)[None, :]).astype(
        jnp.int32
    )
    earlier_hits = jnp.cumsum(onehot, axis=0) - onehot
    slot_index = jnp.sum(earlier_hits * onehot, axis=1)
    return (flat_routes * capacity + slot_index).reshape(route_block.shape)


def pick_matrix(targets, slot_total):
    slot_hits = targets[None, :, :] == jnp.arange(slot_total, dtype=jnp.int32)[:, None, None]
    return jnp.sum(slot_hits.astype(jnp.int32), axis=2).astype(jnp.bfloat16)


def rms_rows(row_block, gain_vector):
    floated = row_block.astype(jnp.float32)
    inverse_rms = lax.rsqrt(jnp.mean(floated * floated, axis=1, keepdims=True) + EPSILON)
    return (floated * inverse_rms * gain_vector[None, :]).astype(jnp.bfloat16)


def expert_apply(row_piece, gate_weight, up_weight, down_weight):
    gate_part = jnp.dot(row_piece, gate_weight, preferred_element_type=jnp.float32)
    up_part = jnp.dot(row_piece, up_weight, preferred_element_type=jnp.float32)
    hidden_units = (jax.nn.silu(gate_part) * up_part).astype(jnp.bfloat16)
    return jnp.dot(hidden_units, down_weight, preferred_element_type=jnp.float32)


def local_slotted(
    lru_input,
    gate_input,
    documents,
    conv_taps,
    rate_weight,
    inlet_weight,
    decay_param,
    lru_gain,
    out_weight,
    residual,
    ffn_gain,
    routes,
    route_weights,
    w_gate,
    w_up,
    w_down,
):
    positions = lru_input.shape[0]
    channels = lru_input.shape[1]
    model_width = residual.shape[1]
    reach_back = conv_taps.shape[0] - 1
    tail_rows, tail_docs = shifted(
        (lru_input[positions - reach_back :], documents[positions - reach_back :] + 1), "sp", 1
    )
    prior_docs = jnp.concatenate([tail_docs - 1, documents])
    padded_input = jnp.concatenate([tail_rows, lru_input], axis=0)
    conv_sum = jnp.zeros((positions, channels), jnp.float32)
    for tap_index in range(reach_back + 1):
        same_doc = (prior_docs[tap_index : tap_index + positions] == documents).astype(jnp.float32)[
            :, None
        ]
        conv_sum = (
            conv_sum
            + padded_input[tap_index : tap_index + positions].astype(jnp.float32)
            * conv_taps[tap_index].astype(jnp.float32)[None, :]
            * same_doc
        )
    convolved = conv_sum.astype(jnp.bfloat16)
    grouped = convolved.reshape(positions, rate_weight.shape[0], rate_weight.shape[1])
    rate_gate = jax.nn.sigmoid(
        jnp.einsum(
            "tnc,ncd->tnd", grouped, rate_weight, preferred_element_type=jnp.float32
        ).reshape(positions, channels)
    )
    inlet_gate = jax.nn.sigmoid(
        jnp.einsum(
            "tnc,ncd->tnd", grouped, inlet_weight, preferred_element_type=jnp.float32
        ).reshape(positions, channels)
    )
    log_decay = -RATE_SCALE * rate_gate * jax.nn.softplus(-decay_param)[None, :]
    starts = (prior_docs[reach_back - 1 : reach_back - 1 + positions] != documents)[:, None]
    decay_step = jnp.where(starts, 0.0, jnp.exp(log_decay))
    norm_factor = jnp.where(starts, 1.0, jnp.sqrt(-jnp.expm1(2.0 * log_decay)))
    drive_term = norm_factor * inlet_gate * convolved.astype(jnp.float32)
    decay_run, local_state = lax.associative_scan(join_runs, (decay_step, drive_term), axis=0)
    carried = carried_in(
        (decay_run[positions - 1], local_state[positions - 1]),
        "sp",
        join_runs,
        (jnp.ones((channels,), jnp.float32), jnp.zeros((channels,), jnp.float32)),
    )
    hidden_state = local_state + decay_run * carried[1][None, :]
    square_sums = lax.psum(jnp.sum(hidden_state * hidden_state, axis=1), "tp")
    inverse_rms = lax.rsqrt(square_sums[:, None] / (channels * lax.axis_size("tp")) + EPSILON)
    mixer_rows = (
        hidden_state * inverse_rms * lru_gain[None, :] * jax.nn.gelu(gate_input.astype(jnp.float32))
    ).astype(jnp.bfloat16)
    tp_count = lax.axis_size("tp")
    tp_here = lax.axis_index("tp")
    expert_count = lax.axis_size("sp")
    route_rows = positions // tp_count
    top_count = routes.shape[1]
    capacity = 2 * top_count * route_rows // expert_count
    slot_total = expert_count * capacity
    projected = lax.psum_scatter(
        jnp.dot(mixer_rows, out_weight, preferred_element_type=jnp.float32).astype(jnp.bfloat16),
        "tp",
        scatter_dimension=0,
        tiled=True,
    ).astype(jnp.float32)
    own_rows = (
        lax.dynamic_slice_in_dim(residual, tp_here * route_rows, route_rows, 0).astype(jnp.float32)
        + projected
    ).astype(jnp.bfloat16)
    own_routes = lax.dynamic_slice_in_dim(routes, tp_here * route_rows, route_rows, 0)
    targets = slot_targets(own_routes, expert_count, capacity)
    outgoing = jnp.dot(
        pick_matrix(targets, slot_total),
        rms_rows(own_rows, ffn_gain),
        preferred_element_type=jnp.float32,
    ).astype(jnp.bfloat16)
    arrived = lax.all_to_all(
        outgoing.reshape(expert_count, capacity, model_width),
        "sp",
        split_axis=0,
        concat_axis=0,
        tiled=True,
    )
    partial_out = expert_apply(
        lax.all_gather(arrived.reshape(slot_total, model_width), "tp", axis=0, tiled=True),
        w_gate[0],
        w_up[0],
        w_down[0],
    )
    expert_out = lax.psum_scatter(
        partial_out.astype(jnp.bfloat16), "tp", scatter_dimension=0, tiled=True
    )
    returned = lax.all_to_all(
        expert_out.reshape(expert_count, capacity, model_width),
        "sp",
        split_axis=0,
        concat_axis=0,
        tiled=True,
    )
    picked = returned.reshape(slot_total, model_width)[targets.reshape(-1)].astype(jnp.float32)
    picked = picked.reshape(route_rows, top_count, model_width)
    own_weights = lax.dynamic_slice_in_dim(route_weights, tp_here * route_rows, route_rows, 0)
    routed = jnp.sum(picked * own_weights[:, :, None], axis=1)
    return (own_rows.astype(jnp.float32) + routed).astype(jnp.bfloat16)


def local(*arrays):
    positions, top_count = arrays[11].shape
    shards = lax.axis_size("sp")
    route_rows = positions // lax.axis_size("tp")
    dense = shards == PLANE and 2 * top_count * route_rows // shards >= route_rows
    return (local_dense if dense else local_slotted)(*arrays)


def solution(mesh):
    return jax.shard_map(
        local,
        mesh=mesh,
        in_specs=(
            P("sp", "tp"),
            P("sp", "tp"),
            P("sp"),
            P(None, "tp"),
            P("tp", None, None),
            P("tp", None, None),
            P("tp"),
            P("tp"),
            P("tp", None),
            P("sp", None),
            P(),
            P("sp", None),
            P("sp", None),
            P("sp", None, "tp"),
            P("sp", None, "tp"),
            P("sp", "tp", None),
        ),
        out_specs=P(("sp", "tp"), None),
        check_vma=False,
    )
```

```python
import functools

import jax
import jax.numpy as jnp
from jax import lax
from jax.experimental import pallas as pl
from jax.experimental.pallas import tpu as pltpu
from jax.sharding import PartitionSpec as P

EPSILON = 1e-06
RATE_SCALE = 8.0
LANES = 128
SUBLANES = 8
CORES = 2
PLANE = 4


F32 = jnp.float32
BF16 = jnp.bfloat16


def vmem_call(kernel, outs, args, scratch=(), limit_mib=4):
    spec = pl.BlockSpec(memory_space=pltpu.VMEM)
    return pl.pallas_call(
        kernel,
        in_specs=[spec] * len(args),
        out_specs=[spec] * len(outs),
        out_shape=[jax.ShapeDtypeStruct(shape, dtype) for shape, dtype in outs],
        scratch_shapes=[pltpu.VMEM(shape, dtype) for shape, dtype in scratch],
        compiler_params=pltpu.CompilerParams(vmem_limit_bytes=limit_mib << 20),
    )(*[pltpu.with_memory_space_constraint(arg, pltpu.VMEM) for arg in args])


def place():
    tp_here = lax.axis_index("tp")
    return lax.axis_index("sp"), tp_here // CORES, tp_here % CORES


def flip(value, axis, distance):
    return lax.ppermute(value, axis, [(i, i ^ distance) for i in range(lax.axis_size(axis))])


def flip_z(value, distance):
    return flip(value, "tp", distance * CORES)


def column(row):
    return jnp.transpose(jnp.broadcast_to(row, (LANES, row.shape[1])))


def one_minus_exp(value):
    series = jnp.ones_like(value)
    for order in range(7, 1, -1):
        series = 1.0 + value * series * (1.0 / order)
    return jnp.where(value > -0.35, -value * series, 1.0 - jnp.exp(value))


def scan_rows(decay, drive):
    rows = decay.shape[0]
    row_ids = lax.broadcasted_iota(jnp.int32, decay.shape, 0)
    distance = 1
    while distance < rows:
        if distance < SUBLANES:
            head = row_ids < distance
            earlier_decay = jnp.where(head, 1.0, pltpu.roll(decay, distance, 0))
            earlier_drive = jnp.where(head, 0.0, pltpu.roll(drive, distance, 0))
            drive = drive + decay * earlier_drive
            decay = decay * earlier_decay
        else:
            late_drive = drive[distance:] + decay[distance:] * drive[: rows - distance]
            late_decay = decay[distance:] * decay[: rows - distance]
            drive = jnp.concatenate([drive[:distance], late_drive], axis=0)
            decay = jnp.concatenate([decay[:distance], late_decay], axis=0)
        distance *= 2
    return decay, drive


def lru_kernel(
    rows_in, gate_in, tail, docs, taps, rate_w, inlet_w, decay_in, gain, routes, route_w,
    state_out, run_out, mix_out, *rest,
):
    *messages, padded, doc_cols = rest
    positions, channels = rows_in.shape
    reach = taps.shape[0] - 1
    first = SUBLANES - reach
    padded[0:SUBLANES] = tail[0:SUBLANES]
    padded[SUBLANES:] = rows_in[...].astype(F32)
    doc_cols[0:SUBLANES] = column(tail[SUBLANES : SUBLANES + 1, 0:LANES])[LANES - SUBLANES :]
    doc_cols[SUBLANES:] = column(docs[...].astype(F32) + 1.0)
    own_doc = doc_cols[SUBLANES:]
    starts = doc_cols[SUBLANES - 1 : SUBLANES - 1 + positions] != own_doc
    for group in range(channels // LANES):
        lanes = slice(group * LANES, (group + 1) * LANES)
        conv = jnp.zeros((positions, LANES), F32)
        for tap in range(reach + 1):
            shifted_rows = padded[first + tap : first + tap + positions, lanes]
            if tap < reach:
                same = doc_cols[first + tap : first + tap + positions] == own_doc
                shifted_rows = jnp.where(same, shifted_rows, 0.0)
            conv = conv + shifted_rows * taps[tap : tap + 1, lanes].astype(F32)
        conv = conv.astype(BF16)
        rate = jax.nn.sigmoid(jnp.dot(conv, rate_w[group], preferred_element_type=F32))
        inlet = jax.nn.sigmoid(jnp.dot(conv, inlet_w[group], preferred_element_type=F32))
        negated = -decay_in[0:1, lanes]
        soft = jnp.maximum(negated, 0.0) + jnp.log1p(jnp.exp(-jnp.abs(negated)))
        log_decay = -RATE_SCALE * rate * soft
        decay = jnp.where(starts, 0.0, jnp.exp(log_decay))
        norm = jnp.where(starts, 1.0, jnp.sqrt(one_minus_exp(2.0 * log_decay)))
        run, state = scan_rows(decay, norm * inlet * conv.astype(F32))
        state_out[:, lanes] = state
        run_out[:, lanes] = run
        mix_out[:, lanes] = jax.nn.gelu(gate_in[:, lanes].astype(F32)) * gain[0:1, lanes]
        for message in messages:
            message[0:1, lanes] = run[positions - 1 :]
            message[1:2, lanes] = state[positions - 1 :]
    shard, _, _ = place()
    for k, message in enumerate(messages):
        dense = jnp.zeros((1, positions), F32)
        for choice in range(routes.shape[0]):
            chosen = routes[choice : choice + 1] == (shard ^ k)
            dense = dense + jnp.where(chosen, route_w[choice : choice + 1], 0.0)
        message[2:3, 0:positions] = dense


def split_sum(total):
    lane_ids = lax.broadcasted_iota(jnp.int32, (total.shape[0], LANES), 1)
    high = total.astype(BF16).astype(F32)
    low = (total - high).astype(BF16).astype(F32)
    return jnp.where(lane_ids == 0, high, jnp.where(lane_ids == 1, low, 0.0)).astype(BF16)


def joined_sum(lanes):
    lanes = lanes.astype(F32)
    return lanes[:, 0:1] + lanes[:, 1:2]


def mix_kernel(state, run, mix, *rest, block):
    *messages, keep, send, stacked, mixed = rest
    channels = state.shape[1]
    for k, message in enumerate(messages):
        stacked[k] = message[...]
    shard, _, core = place()

    def hop(position, carried):
        run_state = stacked[position ^ shard]
        return run_state[0:1, :channels] * carried + run_state[1:2, :channels]

    carried = lax.fori_loop(0, shard, hop, jnp.zeros((1, channels), F32))
    hidden = state[...] + run[...] * carried
    mixed[:, :channels] = (hidden * mix[...]).astype(BF16)
    mixed[:, channels:] = split_sum(jnp.sum(hidden * hidden, axis=1, keepdims=True))
    for z in range(keep.shape[0] // block):
        rows = slice(z * block, (z + 1) * block)
        keep[rows] = mixed[pl.ds(pl.multiple_of((CORES * z + core) * block, block), block)]
        send[rows] = mixed[pl.ds(pl.multiple_of((CORES * z + 1 - core) * block, block), block)]


def project_kernel(keep, other, own_w, other_w, *rest, block):
    *outs, own_rows, other_rows = rest
    channels, width = own_w.shape
    _, depth, _ = place()
    for k in range(len(outs)):
        rows = slice(k * block, (k + 1) * block)
        source = pl.ds(pl.multiple_of((depth ^ k) * block, block), block)
        own_rows[rows] = keep[source]
        other_rows[rows] = other[source]
    squares = split_sum(joined_sum(own_rows[:, channels:]) + joined_sum(other_rows[:, channels:]))
    product = jnp.dot(own_rows[:, :channels], own_w[...], preferred_element_type=F32)
    product = product + jnp.dot(other_rows[:, :channels], other_w[...], preferred_element_type=F32)
    for k, out in enumerate(outs):
        rows = slice(k * block, (k + 1) * block)
        out[:, :width] = product[rows].astype(BF16)
        out[:, width:] = squares[rows]


def norm_kernel(residual, gain, *rest, channels_total):
    *parts, after_out, normed_out = rest
    width = residual.shape[1]
    block = after_out.shape[0]
    own = pl.ds(pl.multiple_of(lax.axis_index("tp") * block, block), block)
    total = sum(part[:, :width].astype(F32) for part in parts)
    squares = sum(joined_sum(part[:, width:]) for part in parts)
    projected = total * lax.rsqrt(squares / channels_total + EPSILON)
    after = (residual[own].astype(F32) + projected).astype(BF16)
    after_out[...] = after
    floated = after.astype(F32)
    inverse_rms = lax.rsqrt(jnp.mean(floated * floated, axis=1, keepdims=True) + EPSILON)
    normed_out[...] = (floated * inverse_rms * gain[...]).astype(BF16)


def expert_kernel(*refs, labels, block, tile, out_tile):
    pieces, refs = refs[: len(labels)], refs[len(labels) :]
    messages, refs = refs[:PLANE], refs[PLANE:]
    (own_gate, other_gate, own_up, other_up, own_down, other_down), refs = refs[:6], refs[6:]
    outs, (tokens, weight_cols, weights, hidden) = refs[: len(labels)], refs[len(labels) :]
    half, width = own_down.shape
    positions = weight_cols.shape[1]
    _, depth, core = place()
    for k in range(PLANE):
        weight_cols[k] = column(messages[k][2:3, :positions])
    at = 0
    for piece, (z_flip, planes) in zip(pieces, labels):
        tokens[at : at + len(planes) * block] = piece[...]
        source = (CORES * (depth ^ z_flip) + core) * block
        for k in planes:
            weights[at : at + block] = weight_cols[k, pl.ds(pl.multiple_of(source, block), block)]
            at += block

    for base, gate_w, up_w in ((0, own_gate, own_up), (half, other_gate, other_up)):

        def hide(index, _):
            spot = pl.multiple_of(index * tile, LANES)
            gate = jnp.dot(tokens[...], gate_w[:, pl.ds(spot, tile)], preferred_element_type=F32)
            up = jnp.dot(tokens[...], up_w[:, pl.ds(spot, tile)], preferred_element_type=F32)
            spot = pl.multiple_of(base + spot, LANES)
            hidden[:, pl.ds(spot, tile)] = (jax.nn.silu(gate) * up).astype(BF16)
            return _

        lax.fori_loop(0, half // tile, hide, 0)

    def lower(index, _):
        cols = pl.ds(pl.multiple_of(index * out_tile, LANES), out_tile)
        product = jnp.dot(hidden[:, :half], own_down[:, cols], preferred_element_type=F32)
        product = product + jnp.dot(hidden[:, half:], other_down[:, cols], preferred_element_type=F32)
        scale = jnp.concatenate([weights[...]] * (out_tile // LANES), axis=1)
        scaled = (product * scale).astype(BF16)
        at = 0
        for out in outs:
            out[:, cols] = scaled[at : at + out.shape[0]]
            at += out.shape[0]
        return _

    lax.fori_loop(0, width // out_tile, lower, 0)


def run_experts(pieces, labels, messages, weights, block):
    half, width = weights[-1].shape
    rows = sum(piece.shape[0] for piece in pieces)
    positions = block * lax.axis_size("tp")
    return vmem_call(
        functools.partial(
            expert_kernel, labels=labels, block=block, tile=half, out_tile=width // 2
        ),
        [(piece.shape, BF16) for piece in pieces],
        [*pieces, *messages, *weights],
        scratch=[
            ((rows, width), BF16),
            ((PLANE, positions, LANES), F32),
            ((rows, LANES), F32),
            ((rows, 2 * half), BF16),
        ],
        limit_mib=10,
    )


def local_dense(
    lru_input, gate_input, documents, conv_taps, rate_weight, inlet_weight, decay_param, lru_gain,
    out_weight, residual, ffn_gain, routes, route_weights, w_gate, w_up, w_down,
):
    positions, channels = lru_input.shape
    width = residual.shape[1]
    tp_count = lax.axis_size("tp")
    depths = tp_count // CORES
    block = positions // tp_count
    span = max(positions, channels)

    last_rows = lru_input[positions - SUBLANES :].astype(F32)
    last_docs = (documents[positions - LANES :] + 1).astype(F32)[None, :]
    last_docs = jnp.pad(last_docs, ((0, 0), (0, channels - LANES)))
    tail = lax.ppermute(
        jnp.concatenate([last_rows, last_docs], axis=0),
        "sp",
        [(i, i + 1) for i in range(PLANE - 1)],
    )
    swapped = [flip(value, "tp", 1) for value in (out_weight, w_gate[0], w_up[0], w_down[0])]

    state, run, mix, *messages = vmem_call(
        lru_kernel,
        [((positions, channels), F32)] * 3 + [((SUBLANES, span), F32)] * PLANE,
        [
            lru_input, gate_input, tail, documents[None, :], conv_taps, rate_weight, inlet_weight,
            decay_param[None, :], lru_gain[None, :], routes.T, route_weights.T,
        ],
        scratch=[
            ((SUBLANES + positions, channels), F32),
            ((SUBLANES + positions, LANES), F32),
        ],
    )
    messages = [messages[0]] + [flip(messages[k], "sp", k) for k in range(1, PLANE)]

    half_rows = positions // CORES
    packed = (half_rows, channels + LANES)
    keep, send = vmem_call(
        functools.partial(mix_kernel, block=block),
        [(packed, BF16)] * 2,
        [state, run, mix, *messages],
        scratch=[((PLANE, SUBLANES, span), F32), ((positions, channels + LANES), BF16)],
    )
    parts = vmem_call(
        functools.partial(project_kernel, block=block),
        [((block, width + LANES), BF16)] * depths,
        [keep, flip(send, "tp", 1), out_weight, swapped[0]],
        scratch=[(packed, BF16)] * 2,
    )
    parts = [parts[0]] + [flip_z(parts[k], k) for k in range(1, depths)]
    after, normed = vmem_call(
        functools.partial(norm_kernel, channels_total=channels * tp_count),
        [((block, width), BF16)] * 2,
        [residual, ffn_gain[None, :], *parts],
    )

    weights = (w_gate[0], swapped[1], w_up[0], swapped[2], w_down[0], swapped[3])
    rows_at = [normed] + [flip_z(normed, k) for k in range(1, depths)]
    finished = []
    for chunk in range(0, depths, 2):
        pieces, labels, orders = [], [], []
        for z_flip in range(chunk, min(chunk + 2, depths)):
            near, far = (1, 2) if z_flip % 2 == 0 else (2, 1)
            pair = jnp.concatenate([rows_at[z_flip], flip(rows_at[z_flip], "sp", near)], axis=0)
            pieces += [pair, flip(pair, "sp", far)]
            labels += [(z_flip, (0, near)), (z_flip, (far, 3))]
            orders.append((near, far))
        outs = run_experts(pieces, tuple(labels), messages, weights, block)
        for index, (near, far) in enumerate(orders):
            summed = outs[2 * index].astype(F32) + flip(outs[2 * index + 1], "sp", far).astype(F32)
            crossing = flip(summed[block:].astype(BF16), "sp", near)
            finished.append((summed[:block].astype(BF16).astype(F32) + crossing.astype(F32)).astype(BF16))
    total = after.astype(F32) + finished[0].astype(F32)
    for k in range(1, depths):
        total = total + flip_z(finished[k], k).astype(F32)
    return total.astype(BF16)


def shifted(block, axis, distance):
    devices = range(lax.axis_size(axis))
    route = [(i - distance, i) for i in devices if i - distance in devices]
    return lax.ppermute(block, axis, route)


def carried_in(value, axis, join, neutral):
    count, mine = (lax.axis_size(axis), lax.axis_index(axis))
    pieces = jax.tree.map(lambda part: lax.all_gather(part, axis), value)
    so_far = jax.tree.map(
        lambda part, zero: jnp.full_like(part, 0) + jnp.asarray(zero, part.dtype), value, neutral
    )

    def hop(position, so_far):
        longer = join(so_far, jax.tree.map(lambda part: part[position], pieces))
        return jax.tree.map(lambda new, old: jnp.where(position < mine, new, old), longer, so_far)

    return lax.fori_loop(0, count - 1, hop, so_far)


def join_runs(earlier_run, later_run):
    return (earlier_run[0] * later_run[0], later_run[0] * earlier_run[1] + later_run[1])


def slot_targets(route_block, expert_count, capacity):
    flat_routes = route_block.reshape(-1)
    onehot = (flat_routes[:, None] == jnp.arange(expert_count, dtype=jnp.int32)[None, :]).astype(
        jnp.int32
    )
    earlier_hits = jnp.cumsum(onehot, axis=0) - onehot
    slot_index = jnp.sum(earlier_hits * onehot, axis=1)
    return (flat_routes * capacity + slot_index).reshape(route_block.shape)


def pick_matrix(targets, slot_total):
    slot_hits = targets[None, :, :] == jnp.arange(slot_total, dtype=jnp.int32)[:, None, None]
    return jnp.sum(slot_hits.astype(jnp.int32), axis=2).astype(jnp.bfloat16)


def rms_rows(row_block, gain_vector):
    floated = row_block.astype(jnp.float32)
    inverse_rms = lax.rsqrt(jnp.mean(floated * floated, axis=1, keepdims=True) + EPSILON)
    return (floated * inverse_rms * gain_vector[None, :]).astype(jnp.bfloat16)


def expert_apply(row_piece, gate_weight, up_weight, down_weight):
    gate_part = jnp.dot(row_piece, gate_weight, preferred_element_type=jnp.float32)
    up_part = jnp.dot(row_piece, up_weight, preferred_element_type=jnp.float32)
    hidden_units = (jax.nn.silu(gate_part) * up_part).astype(jnp.bfloat16)
    return jnp.dot(hidden_units, down_weight, preferred_element_type=jnp.float32)


def local_slotted(
    lru_input,
    gate_input,
    documents,
    conv_taps,
    rate_weight,
    inlet_weight,
    decay_param,
    lru_gain,
    out_weight,
    residual,
    ffn_gain,
    routes,
    route_weights,
    w_gate,
    w_up,
    w_down,
):
    positions = lru_input.shape[0]
    channels = lru_input.shape[1]
    model_width = residual.shape[1]
    reach_back = conv_taps.shape[0] - 1
    tail_rows, tail_docs = shifted(
        (lru_input[positions - reach_back :], documents[positions - reach_back :] + 1), "sp", 1
    )
    prior_docs = jnp.concatenate([tail_docs - 1, documents])
    padded_input = jnp.concatenate([tail_rows, lru_input], axis=0)
    conv_sum = jnp.zeros((positions, channels), jnp.float32)
    for tap_index in range(reach_back + 1):
        same_doc = (prior_docs[tap_index : tap_index + positions] == documents).astype(jnp.float32)[
            :, None
        ]
        conv_sum = (
            conv_sum
            + padded_input[tap_index : tap_index + positions].astype(jnp.float32)
            * conv_taps[tap_index].astype(jnp.float32)[None, :]
            * same_doc
        )
    convolved = conv_sum.astype(jnp.bfloat16)
    grouped = convolved.reshape(positions, rate_weight.shape[0], rate_weight.shape[1])
    rate_gate = jax.nn.sigmoid(
        jnp.einsum(
            "tnc,ncd->tnd", grouped, rate_weight, preferred_element_type=jnp.float32
        ).reshape(positions, channels)
    )
    inlet_gate = jax.nn.sigmoid(
        jnp.einsum(
            "tnc,ncd->tnd", grouped, inlet_weight, preferred_element_type=jnp.float32
        ).reshape(positions, channels)
    )
    log_decay = -RATE_SCALE * rate_gate * jax.nn.softplus(-decay_param)[None, :]
    starts = (prior_docs[reach_back - 1 : reach_back - 1 + positions] != documents)[:, None]
    decay_step = jnp.where(starts, 0.0, jnp.exp(log_decay))
    norm_factor = jnp.where(starts, 1.0, jnp.sqrt(-jnp.expm1(2.0 * log_decay)))
    drive_term = norm_factor * inlet_gate * convolved.astype(jnp.float32)
    decay_run, local_state = lax.associative_scan(join_runs, (decay_step, drive_term), axis=0)
    carried = carried_in(
        (decay_run[positions - 1], local_state[positions - 1]),
        "sp",
        join_runs,
        (jnp.ones((channels,), jnp.float32), jnp.zeros((channels,), jnp.float32)),
    )
    hidden_state = local_state + decay_run * carried[1][None, :]
    square_sums = lax.psum(jnp.sum(hidden_state * hidden_state, axis=1), "tp")
    inverse_rms = lax.rsqrt(square_sums[:, None] / (channels * lax.axis_size("tp")) + EPSILON)
    mixer_rows = (
        hidden_state * inverse_rms * lru_gain[None, :] * jax.nn.gelu(gate_input.astype(jnp.float32))
    ).astype(jnp.bfloat16)
    tp_count = lax.axis_size("tp")
    tp_here = lax.axis_index("tp")
    expert_count = lax.axis_size("sp")
    route_rows = positions // tp_count
    top_count = routes.shape[1]
    capacity = 2 * top_count * route_rows // expert_count
    slot_total = expert_count * capacity
    projected = lax.psum_scatter(
        jnp.dot(mixer_rows, out_weight, preferred_element_type=jnp.float32).astype(jnp.bfloat16),
        "tp",
        scatter_dimension=0,
        tiled=True,
    ).astype(jnp.float32)
    own_rows = (
        lax.dynamic_slice_in_dim(residual, tp_here * route_rows, route_rows, 0).astype(jnp.float32)
        + projected
    ).astype(jnp.bfloat16)
    own_routes = lax.dynamic_slice_in_dim(routes, tp_here * route_rows, route_rows, 0)
    targets = slot_targets(own_routes, expert_count, capacity)
    outgoing = jnp.dot(
        pick_matrix(targets, slot_total),
        rms_rows(own_rows, ffn_gain),
        preferred_element_type=jnp.float32,
    ).astype(jnp.bfloat16)
    arrived = lax.all_to_all(
        outgoing.reshape(expert_count, capacity, model_width),
        "sp",
        split_axis=0,
        concat_axis=0,
        tiled=True,
    )
    partial_out = expert_apply(
        lax.all_gather(arrived.reshape(slot_total, model_width), "tp", axis=0, tiled=True),
        w_gate[0],
        w_up[0],
        w_down[0],
    )
    expert_out = lax.psum_scatter(
        partial_out.astype(jnp.bfloat16), "tp", scatter_dimension=0, tiled=True
    )
    returned = lax.all_to_all(
        expert_out.reshape(expert_count, capacity, model_width),
        "sp",
        split_axis=0,
        concat_axis=0,
        tiled=True,
    )
    picked = returned.reshape(slot_total, model_width)[targets.reshape(-1)].astype(jnp.float32)
    picked = picked.reshape(route_rows, top_count, model_width)
    own_weights = lax.dynamic_slice_in_dim(route_weights, tp_here * route_rows, route_rows, 0)
    routed = jnp.sum(picked * own_weights[:, :, None], axis=1)
    return (own_rows.astype(jnp.float32) + routed).astype(jnp.bfloat16)


def local(*arrays):
    positions, top_count = arrays[11].shape
    shards = lax.axis_size("sp")
    route_rows = positions // lax.axis_size("tp")
    dense = shards == PLANE and 2 * top_count * route_rows // shards >= route_rows
    return (local_dense if dense else local_slotted)(*arrays)


def solution(mesh):
    return jax.shard_map(
        local,
        mesh=mesh,
        in_specs=(
            P("sp", "tp"),
            P("sp", "tp"),
            P("sp"),
            P(None, "tp"),
            P("tp", None, None),
            P("tp", None, None),
            P("tp"),
            P("tp"),
            P("tp", None),
            P("sp", None),
            P(),
            P("sp", None),
            P("sp", None),
            P("sp", None, "tp"),
            P("sp", None, "tp"),
            P("sp", "tp", None),
        ),
        out_specs=P(("sp", "tp"), None),
        check_vma=False,
    )
```

```python
import functools

import jax
import jax.numpy as jnp
from jax import lax
from jax.experimental import pallas as pl
from jax.experimental.pallas import tpu as pltpu
from jax.sharding import PartitionSpec as P

EPSILON = 1e-06
RATE_SCALE = 8.0
LANES = 128
SUBLANES = 8
CORES = 2
PLANE = 4


F32 = jnp.float32
BF16 = jnp.bfloat16


def vmem_call(kernel, outs, args, scratch=(), limit_mib=4, far_args=()):
    near, far = (pl.BlockSpec(memory_space=space) for space in (pltpu.VMEM, pltpu.HBM))
    return pl.pallas_call(
        kernel,
        in_specs=[far] * len(far_args) + [near] * len(args),
        out_specs=[near] * len(outs),
        out_shape=[jax.ShapeDtypeStruct(shape, dtype) for shape, dtype in outs],
        scratch_shapes=[
            pltpu.VMEM(*what) if isinstance(what, tuple) else what for what in scratch
        ],
        compiler_params=pltpu.CompilerParams(vmem_limit_bytes=limit_mib << 20),
    )(
        *[pltpu.with_memory_space_constraint(arg, pltpu.HBM) for arg in far_args],
        *[pltpu.with_memory_space_constraint(arg, pltpu.VMEM) for arg in args],
    )


def place():
    tp_here = lax.axis_index("tp")
    return lax.axis_index("sp"), tp_here // CORES, tp_here % CORES


def flip(value, axis, distance):
    return lax.ppermute(value, axis, [(i, i ^ distance) for i in range(lax.axis_size(axis))])


def flip_z(value, distance):
    return flip(value, "tp", distance * CORES)


def column(row):
    return jnp.transpose(jnp.broadcast_to(row, (LANES, row.shape[1])))


def one_minus_exp(value):
    series = jnp.ones_like(value)
    for order in range(7, 1, -1):
        series = 1.0 + value * series * (1.0 / order)
    return jnp.where(value > -0.35, -value * series, 1.0 - jnp.exp(value))


def scan_rows(decay, drive):
    rows = decay.shape[0]
    row_ids = lax.broadcasted_iota(jnp.int32, decay.shape, 0)
    distance = 1
    while distance < rows:
        if distance < SUBLANES:
            head = row_ids < distance
            earlier_decay = jnp.where(head, 1.0, pltpu.roll(decay, distance, 0))
            earlier_drive = jnp.where(head, 0.0, pltpu.roll(drive, distance, 0))
            drive = drive + decay * earlier_drive
            decay = decay * earlier_decay
        else:
            late_drive = drive[distance:] + decay[distance:] * drive[: rows - distance]
            late_decay = decay[distance:] * decay[: rows - distance]
            drive = jnp.concatenate([drive[:distance], late_drive], axis=0)
            decay = jnp.concatenate([decay[:distance], late_decay], axis=0)
        distance *= 2
    return decay, drive


def gated_terms(conv, starts, rate_w, inlet_w, decay_in):
    conv = conv.astype(BF16)
    rate = jax.nn.sigmoid(jnp.dot(conv, rate_w, preferred_element_type=F32))
    inlet = jax.nn.sigmoid(jnp.dot(conv, inlet_w, preferred_element_type=F32))
    negated = -decay_in
    soft = jnp.maximum(negated, 0.0) + jnp.log1p(jnp.exp(-jnp.abs(negated)))
    log_decay = -RATE_SCALE * rate * soft
    decay = jnp.where(starts, 0.0, jnp.exp(log_decay))
    norm = jnp.where(starts, 1.0, jnp.sqrt(one_minus_exp(2.0 * log_decay)))
    return decay, norm * inlet * conv.astype(F32)


def convolve(padded, docs, taps, at, count, lanes):
    reach = taps.shape[0] - 1
    own_doc = docs[at : at + count]
    conv = jnp.zeros((count, LANES), F32)
    for tap in range(reach + 1):
        source = slice(at - reach + tap, at - reach + tap + count)
        rows = padded[source, lanes]
        if tap < reach:
            rows = jnp.where(docs[source] == own_doc, rows, 0.0)
        conv = conv + rows * taps[tap : tap + 1, lanes].astype(F32)
    return conv, docs[at - 1 : at - 1 + count] != own_doc


FIRST, LAST, FIRST_DOCS, LAST_DOCS = (SUBLANES * i for i in range(1, 5))
MESSAGE_ROWS = 5 * SUBLANES


def lru_kernel(*refs):
    far, refs = refs[:12], refs[12:]
    (state_out, run_out, mix_out), refs = refs[:3], refs[3:]
    messages, refs = refs[:PLANE], refs[PLANE:]
    (taps, rate_w, inlet_w, decay_in, out_w, residual), refs = refs[:6], refs[6:]
    rows_in, gate_in, docs, gain, routes, route_w, padded, doc_cols, sems = refs
    block = residual.shape[0]
    own = pl.ds(pl.multiple_of(lax.axis_index("tp") * block, block), block)
    sources = [*far[:11], far[11].at[own]]
    targets = (
        rows_in, docs, taps, rate_w, inlet_w, decay_in, gate_in, gain, routes, route_w, out_w, residual,
    )
    copies = [
        pltpu.make_async_copy(source, target, sems.at[i])
        for i, (source, target) in enumerate(zip(sources, targets))
    ]
    for copy in copies:
        copy.start()
    for copy in copies[:-2]:
        copy.wait()
    positions, channels = rows_in.shape
    reach = taps.shape[0] - 1
    padded[0:SUBLANES] = jnp.zeros((SUBLANES, channels), F32)
    padded[SUBLANES:] = rows_in[...].astype(F32)
    doc_cols[0:SUBLANES] = jnp.zeros((SUBLANES, LANES), F32)
    doc_cols[SUBLANES:] = column(docs[...].astype(F32) + 1.0)
    later = lax.broadcasted_iota(jnp.int32, (positions, LANES), 0) >= reach
    for group in range(channels // LANES):
        lanes = slice(group * LANES, (group + 1) * LANES)
        conv, starts = convolve(padded, doc_cols, taps, SUBLANES, positions, lanes)
        decay, drive = gated_terms(
            conv, starts, rate_w[group], inlet_w[group], decay_in[0:1, lanes]
        )
        run, state = scan_rows(jnp.where(later, decay, 1.0), jnp.where(later, drive, 0.0))
        state_out[:, lanes] = state
        run_out[:, lanes] = run
        for message in messages:
            message[0:1, lanes] = run[positions - 1 :]
            message[1:2, lanes] = state[positions - 1 :]
        mix_out[:, lanes] = jax.nn.gelu(gate_in[:, lanes].astype(F32)) * gain[0:1, lanes]
    shard, _, _ = place()
    for k, message in enumerate(messages):
        dense = jnp.zeros((1, positions), F32)
        for choice in range(routes.shape[0]):
            chosen = routes[choice : choice + 1] == (shard ^ k)
            dense = dense + jnp.where(chosen, route_w[choice : choice + 1], 0.0)
        message[2:3, 0:positions] = dense
        message[FIRST : FIRST + SUBLANES, 0:channels] = padded[SUBLANES : 2 * SUBLANES]
        message[LAST : LAST + SUBLANES, 0:channels] = padded[positions : positions + SUBLANES]
        message[FIRST_DOCS : FIRST_DOCS + SUBLANES, 0:LANES] = doc_cols[SUBLANES : 2 * SUBLANES]
        message[LAST_DOCS : LAST_DOCS + SUBLANES, 0:LANES] = doc_cols[positions : positions + SUBLANES]
    for copy in copies[-2:]:
        copy.wait()


def split_sum(total):
    lane_ids = lax.broadcasted_iota(jnp.int32, (total.shape[0], LANES), 1)
    high = total.astype(BF16).astype(F32)
    low = (total - high).astype(BF16).astype(F32)
    return jnp.where(lane_ids == 0, high, jnp.where(lane_ids == 1, low, 0.0)).astype(BF16)


def joined_sum(lanes):
    lanes = lanes.astype(F32)
    return lanes[:, 0:1] + lanes[:, 1:2]


def mix_kernel(state, run, mix, taps, rate_w, inlet_w, decay_in, *rest, block):
    *messages, keep, send, stacked, edge, edge_docs, terms, heads, hidden, mixed = rest
    channels = state.shape[1]
    reach = taps.shape[0] - 1
    for k, message in enumerate(messages):
        stacked[k] = message[...]
    shard, _, core = place()
    pair = 2 * SUBLANES
    for j in range(PLANE):
        here = stacked.at[j ^ shard]
        at = j * pair
        if j == 0:
            edge[at : at + SUBLANES] = jnp.zeros((SUBLANES, channels), F32)
            edge_docs[at : at + SUBLANES] = jnp.zeros((SUBLANES, LANES), F32)
        else:
            before = stacked.at[(j - 1) ^ shard]
            edge[at : at + SUBLANES] = before[LAST : LAST + SUBLANES, :channels]
            edge_docs[at : at + SUBLANES] = before[LAST_DOCS : LAST_DOCS + SUBLANES, :LANES]
        edge[at + SUBLANES : at + pair] = here[FIRST : FIRST + SUBLANES, :channels]
        edge_docs[at + SUBLANES : at + pair] = here[FIRST_DOCS : FIRST_DOCS + SUBLANES, :LANES]
    for group in range(channels // LANES):
        lanes = slice(group * LANES, (group + 1) * LANES)
        firsts = [
            convolve(edge, edge_docs, taps, j * pair + SUBLANES, SUBLANES, lanes)
            for j in range(PLANE)
        ]
        conv = jnp.concatenate([first[0] for first in firsts], axis=0)
        for j, (_, starts) in enumerate(firsts):
            rows = slice(j * SUBLANES, (j + 1) * SUBLANES)
            heads[j, :, lanes] = jnp.where(starts, 1.0, 0.0)
        starts = jnp.concatenate([heads[j, :, lanes] for j in range(PLANE)], axis=0) > 0.5
        terms[0, :, lanes], terms[1, :, lanes] = gated_terms(
            conv, starts, rate_w[group], inlet_w[group], decay_in[0:1, lanes]
        )
    carried = jnp.zeros((1, channels), F32)
    for j in range(PLANE):
        for row in range(reach):
            at = j * SUBLANES + row
            carried = terms[0, at : at + 1] * carried + terms[1, at : at + 1]
            heads[j, row : row + 1] = carried
        here = stacked.at[j ^ shard]
        carried = here[0:1, :channels] * carried + here[1:2, :channels]
    head = heads[shard]
    hidden[...] = state[...] + run[...] * head[reach - 1 : reach]
    early = lax.broadcasted_iota(jnp.int32, (SUBLANES, channels), 0) < reach
    hidden[0:SUBLANES] = jnp.where(early, head, hidden[0:SUBLANES])
    whole = hidden[...]
    mixed[:, :channels] = (whole * mix[...]).astype(BF16)
    mixed[:, channels:] = split_sum(jnp.sum(whole * whole, axis=1, keepdims=True))
    for z in range(keep.shape[0] // block):
        rows = slice(z * block, (z + 1) * block)
        keep[rows] = mixed[pl.ds(pl.multiple_of((CORES * z + core) * block, block), block)]
        send[rows] = mixed[pl.ds(pl.multiple_of((CORES * z + 1 - core) * block, block), block)]


def project_kernel(keep, other, own_w, other_w, *rest, block):
    *outs, own_rows, other_rows = rest
    channels, width = own_w.shape
    _, depth, _ = place()
    for k in range(len(outs)):
        rows = slice(k * block, (k + 1) * block)
        source = pl.ds(pl.multiple_of((depth ^ k) * block, block), block)
        own_rows[rows] = keep[source]
        other_rows[rows] = other[source]
    squares = split_sum(joined_sum(own_rows[:, channels:]) + joined_sum(other_rows[:, channels:]))
    product = jnp.dot(own_rows[:, :channels], own_w[...], preferred_element_type=F32)
    product = product + jnp.dot(other_rows[:, :channels], other_w[...], preferred_element_type=F32)
    for k, out in enumerate(outs):
        rows = slice(k * block, (k + 1) * block)
        out[:, :width] = product[rows].astype(BF16)
        out[:, width:] = squares[rows]


def norm_kernel(residual, gain, *rest, channels_total):
    *parts, after_out, normed_out = rest
    width = residual.shape[1]
    total = sum(part[:, :width].astype(F32) for part in parts)
    squares = sum(joined_sum(part[:, width:]) for part in parts)
    projected = total * lax.rsqrt(squares / channels_total + EPSILON)
    after = (residual[...].astype(F32) + projected).astype(BF16)
    after_out[...] = after
    floated = after.astype(F32)
    inverse_rms = lax.rsqrt(jnp.mean(floated * floated, axis=1, keepdims=True) + EPSILON)
    normed_out[...] = (floated * inverse_rms * gain[...]).astype(BF16)


def expert_kernel(far_down, *refs, labels, block, tile, out_tile):
    pieces, refs = refs[: len(labels)], refs[len(labels) :]
    messages, refs = refs[:PLANE], refs[PLANE:]
    (own_gate, other_gate, own_up, other_up, other_down), refs = refs[:5], refs[5:]
    outs, refs = refs[: len(labels)], refs[len(labels) :]
    tokens, weight_cols, weights, hidden, own_down, sem = refs
    fetch = pltpu.make_async_copy(far_down, own_down, sem)
    fetch.start()
    half, width = own_down.shape
    positions = weight_cols.shape[1]
    _, depth, core = place()
    for k in range(PLANE):
        weight_cols[k] = column(messages[k][2:3, :positions])
    at = 0
    for piece, (z_flip, planes) in zip(pieces, labels):
        tokens[at : at + len(planes) * block] = piece[...]
        source = (CORES * (depth ^ z_flip) + core) * block
        for k in planes:
            weights[at : at + block] = weight_cols[k, pl.ds(pl.multiple_of(source, block), block)]
            at += block

    for base, gate_w, up_w in ((0, own_gate, own_up), (half, other_gate, other_up)):

        def hide(index, _):
            spot = pl.multiple_of(index * tile, LANES)
            gate = jnp.dot(tokens[...], gate_w[:, pl.ds(spot, tile)], preferred_element_type=F32)
            up = jnp.dot(tokens[...], up_w[:, pl.ds(spot, tile)], preferred_element_type=F32)
            spot = pl.multiple_of(base + spot, LANES)
            hidden[:, pl.ds(spot, tile)] = (jax.nn.silu(gate) * up).astype(BF16)
            return _

        lax.fori_loop(0, half // tile, hide, 0)

    fetch.wait()

    def lower(index, _):
        cols = pl.ds(pl.multiple_of(index * out_tile, LANES), out_tile)
        product = jnp.dot(hidden[:, :half], own_down[:, cols], preferred_element_type=F32)
        product = product + jnp.dot(hidden[:, half:], other_down[:, cols], preferred_element_type=F32)
        scale = jnp.concatenate([weights[...]] * (out_tile // LANES), axis=1)
        scaled = (product * scale).astype(BF16)
        at = 0
        for out in outs:
            out[:, cols] = scaled[at : at + out.shape[0]]
            at += out.shape[0]
        return _

    lax.fori_loop(0, width // out_tile, lower, 0)


def run_experts(pieces, labels, messages, weights, block):
    own_down, *weights = weights
    half, width = own_down.shape
    rows = sum(piece.shape[0] for piece in pieces)
    positions = block * lax.axis_size("tp")
    return vmem_call(
        functools.partial(
            expert_kernel, labels=labels, block=block, tile=half, out_tile=width // 2
        ),
        [(piece.shape, BF16) for piece in pieces],
        [*pieces, *messages, *weights],
        scratch=[
            ((rows, width), BF16),
            ((PLANE, positions, LANES), F32),
            ((rows, LANES), F32),
            ((rows, 2 * half), BF16),
            ((half, width), BF16),
            pltpu.SemaphoreType.DMA,
        ],
        limit_mib=12,
        far_args=[own_down],
    )


def local_dense(
    lru_input, gate_input, documents, conv_taps, rate_weight, inlet_weight, decay_param, lru_gain,
    out_weight, residual, ffn_gain, routes, route_weights, w_gate, w_up, w_down,
):
    positions, channels = lru_input.shape
    width = residual.shape[1]
    tp_count = lax.axis_size("tp")
    depths = tp_count // CORES
    block = positions // tp_count
    span = max(positions, channels)

    swapped = [flip(value, "tp", 1) for value in (out_weight, w_gate[0], w_up[0], w_down[0])]

    state, run, mix, *rest = vmem_call(
        lru_kernel,
        [((positions, channels), F32)] * 3
        + [((MESSAGE_ROWS, span), F32)] * PLANE
        + [
            (conv_taps.shape, BF16), (rate_weight.shape, BF16), (inlet_weight.shape, BF16),
            ((1, channels), F32), (out_weight.shape, BF16), ((block, width), BF16),
        ],
        [],
        scratch=[
            ((positions, channels), BF16),
            ((positions, channels), BF16),
            ((1, positions), jnp.int32),
            ((1, channels), F32),
            (routes.T.shape, jnp.int32),
            (routes.T.shape, F32),
            ((SUBLANES + positions, channels), F32),
            ((SUBLANES + positions, LANES), F32),
            pltpu.SemaphoreType.DMA((12,)),
        ],
        far_args=[
            lru_input, documents[None, :], conv_taps, rate_weight, inlet_weight,
            decay_param[None, :], gate_input, lru_gain[None, :], routes.T, route_weights.T,
            out_weight, residual,
        ],
    )
    messages, (taps, rate_w, inlet_w, decay_in, own_out, own_residual) = rest[:PLANE], rest[PLANE:]
    messages = [messages[0]] + [flip(messages[k], "sp", k) for k in range(1, PLANE)]

    half_rows = positions // CORES
    packed = (half_rows, channels + LANES)
    keep, send = vmem_call(
        functools.partial(mix_kernel, block=block),
        [(packed, BF16)] * 2,
        [state, run, mix, taps, rate_w, inlet_w, decay_in, *messages],
        scratch=[
            ((PLANE, MESSAGE_ROWS, span), F32),
            ((2 * PLANE * SUBLANES, channels), F32),
            ((2 * PLANE * SUBLANES, LANES), F32),
            ((2, PLANE * SUBLANES, channels), F32),
            ((PLANE, SUBLANES, channels), F32),
            ((positions, channels), F32),
            ((positions, channels + LANES), BF16),
        ],
    )
    parts = vmem_call(
        functools.partial(project_kernel, block=block),
        [((block, width + LANES), BF16)] * depths,
        [keep, flip(send, "tp", 1), own_out, swapped[0]],
        scratch=[(packed, BF16)] * 2,
    )
    parts = [parts[0]] + [flip_z(parts[k], k) for k in range(1, depths)]
    after, normed = vmem_call(
        functools.partial(norm_kernel, channels_total=channels * tp_count),
        [((block, width), BF16)] * 2,
        [own_residual, ffn_gain[None, :], *parts],
    )

    weights = (w_down[0], w_gate[0], swapped[1], w_up[0], swapped[2], swapped[3])
    rows_at = [normed] + [flip_z(normed, k) for k in range(1, depths)]
    finished = []
    for chunk in range(0, depths, 2):
        pieces, labels, orders = [], [], []
        for z_flip in range(chunk, min(chunk + 2, depths)):
            near, far = (1, 2) if z_flip % 2 == 0 else (2, 1)
            pair = jnp.concatenate([rows_at[z_flip], flip(rows_at[z_flip], "sp", near)], axis=0)
            pieces += [pair, flip(pair, "sp", far)]
            labels += [(z_flip, (0, near)), (z_flip, (far, 3))]
            orders.append((near, far))
        outs = run_experts(pieces, tuple(labels), messages, weights, block)
        for index, (near, far) in enumerate(orders):
            summed = outs[2 * index].astype(F32) + flip(outs[2 * index + 1], "sp", far).astype(F32)
            crossing = flip(summed[block:].astype(BF16), "sp", near)
            finished.append((summed[:block].astype(BF16).astype(F32) + crossing.astype(F32)).astype(BF16))
    total = after.astype(F32) + finished[0].astype(F32)
    for k in range(1, depths):
        total = total + flip_z(finished[k], k).astype(F32)
    return total.astype(BF16)


def shifted(block, axis, distance):
    devices = range(lax.axis_size(axis))
    route = [(i - distance, i) for i in devices if i - distance in devices]
    return lax.ppermute(block, axis, route)


def carried_in(value, axis, join, neutral):
    count, mine = (lax.axis_size(axis), lax.axis_index(axis))
    pieces = jax.tree.map(lambda part: lax.all_gather(part, axis), value)
    so_far = jax.tree.map(
        lambda part, zero: jnp.full_like(part, 0) + jnp.asarray(zero, part.dtype), value, neutral
    )

    def hop(position, so_far):
        longer = join(so_far, jax.tree.map(lambda part: part[position], pieces))
        return jax.tree.map(lambda new, old: jnp.where(position < mine, new, old), longer, so_far)

    return lax.fori_loop(0, count - 1, hop, so_far)


def join_runs(earlier_run, later_run):
    return (earlier_run[0] * later_run[0], later_run[0] * earlier_run[1] + later_run[1])


def slot_targets(route_block, expert_count, capacity):
    flat_routes = route_block.reshape(-1)
    onehot = (flat_routes[:, None] == jnp.arange(expert_count, dtype=jnp.int32)[None, :]).astype(
        jnp.int32
    )
    earlier_hits = jnp.cumsum(onehot, axis=0) - onehot
    slot_index = jnp.sum(earlier_hits * onehot, axis=1)
    return (flat_routes * capacity + slot_index).reshape(route_block.shape)


def pick_matrix(targets, slot_total):
    slot_hits = targets[None, :, :] == jnp.arange(slot_total, dtype=jnp.int32)[:, None, None]
    return jnp.sum(slot_hits.astype(jnp.int32), axis=2).astype(jnp.bfloat16)


def rms_rows(row_block, gain_vector):
    floated = row_block.astype(jnp.float32)
    inverse_rms = lax.rsqrt(jnp.mean(floated * floated, axis=1, keepdims=True) + EPSILON)
    return (floated * inverse_rms * gain_vector[None, :]).astype(jnp.bfloat16)


def expert_apply(row_piece, gate_weight, up_weight, down_weight):
    gate_part = jnp.dot(row_piece, gate_weight, preferred_element_type=jnp.float32)
    up_part = jnp.dot(row_piece, up_weight, preferred_element_type=jnp.float32)
    hidden_units = (jax.nn.silu(gate_part) * up_part).astype(jnp.bfloat16)
    return jnp.dot(hidden_units, down_weight, preferred_element_type=jnp.float32)


def local_slotted(
    lru_input,
    gate_input,
    documents,
    conv_taps,
    rate_weight,
    inlet_weight,
    decay_param,
    lru_gain,
    out_weight,
    residual,
    ffn_gain,
    routes,
    route_weights,
    w_gate,
    w_up,
    w_down,
):
    positions = lru_input.shape[0]
    channels = lru_input.shape[1]
    model_width = residual.shape[1]
    reach_back = conv_taps.shape[0] - 1
    tail_rows, tail_docs = shifted(
        (lru_input[positions - reach_back :], documents[positions - reach_back :] + 1), "sp", 1
    )
    prior_docs = jnp.concatenate([tail_docs - 1, documents])
    padded_input = jnp.concatenate([tail_rows, lru_input], axis=0)
    conv_sum = jnp.zeros((positions, channels), jnp.float32)
    for tap_index in range(reach_back + 1):
        same_doc = (prior_docs[tap_index : tap_index + positions] == documents).astype(jnp.float32)[
            :, None
        ]
        conv_sum = (
            conv_sum
            + padded_input[tap_index : tap_index + positions].astype(jnp.float32)
            * conv_taps[tap_index].astype(jnp.float32)[None, :]
            * same_doc
        )
    convolved = conv_sum.astype(jnp.bfloat16)
    grouped = convolved.reshape(positions, rate_weight.shape[0], rate_weight.shape[1])
    rate_gate = jax.nn.sigmoid(
        jnp.einsum(
            "tnc,ncd->tnd", grouped, rate_weight, preferred_element_type=jnp.float32
        ).reshape(positions, channels)
    )
    inlet_gate = jax.nn.sigmoid(
        jnp.einsum(
            "tnc,ncd->tnd", grouped, inlet_weight, preferred_element_type=jnp.float32
        ).reshape(positions, channels)
    )
    log_decay = -RATE_SCALE * rate_gate * jax.nn.softplus(-decay_param)[None, :]
    starts = (prior_docs[reach_back - 1 : reach_back - 1 + positions] != documents)[:, None]
    decay_step = jnp.where(starts, 0.0, jnp.exp(log_decay))
    norm_factor = jnp.where(starts, 1.0, jnp.sqrt(-jnp.expm1(2.0 * log_decay)))
    drive_term = norm_factor * inlet_gate * convolved.astype(jnp.float32)
    decay_run, local_state = lax.associative_scan(join_runs, (decay_step, drive_term), axis=0)
    carried = carried_in(
        (decay_run[positions - 1], local_state[positions - 1]),
        "sp",
        join_runs,
        (jnp.ones((channels,), jnp.float32), jnp.zeros((channels,), jnp.float32)),
    )
    hidden_state = local_state + decay_run * carried[1][None, :]
    square_sums = lax.psum(jnp.sum(hidden_state * hidden_state, axis=1), "tp")
    inverse_rms = lax.rsqrt(square_sums[:, None] / (channels * lax.axis_size("tp")) + EPSILON)
    mixer_rows = (
        hidden_state * inverse_rms * lru_gain[None, :] * jax.nn.gelu(gate_input.astype(jnp.float32))
    ).astype(jnp.bfloat16)
    tp_count = lax.axis_size("tp")
    tp_here = lax.axis_index("tp")
    expert_count = lax.axis_size("sp")
    route_rows = positions // tp_count
    top_count = routes.shape[1]
    capacity = 2 * top_count * route_rows // expert_count
    slot_total = expert_count * capacity
    projected = lax.psum_scatter(
        jnp.dot(mixer_rows, out_weight, preferred_element_type=jnp.float32).astype(jnp.bfloat16),
        "tp",
        scatter_dimension=0,
        tiled=True,
    ).astype(jnp.float32)
    own_rows = (
        lax.dynamic_slice_in_dim(residual, tp_here * route_rows, route_rows, 0).astype(jnp.float32)
        + projected
    ).astype(jnp.bfloat16)
    own_routes = lax.dynamic_slice_in_dim(routes, tp_here * route_rows, route_rows, 0)
    targets = slot_targets(own_routes, expert_count, capacity)
    outgoing = jnp.dot(
        pick_matrix(targets, slot_total),
        rms_rows(own_rows, ffn_gain),
        preferred_element_type=jnp.float32,
    ).astype(jnp.bfloat16)
    arrived = lax.all_to_all(
        outgoing.reshape(expert_count, capacity, model_width),
        "sp",
        split_axis=0,
        concat_axis=0,
        tiled=True,
    )
    partial_out = expert_apply(
        lax.all_gather(arrived.reshape(slot_total, model_width), "tp", axis=0, tiled=True),
        w_gate[0],
        w_up[0],
        w_down[0],
    )
    expert_out = lax.psum_scatter(
        partial_out.astype(jnp.bfloat16), "tp", scatter_dimension=0, tiled=True
    )
    returned = lax.all_to_all(
        expert_out.reshape(expert_count, capacity, model_width),
        "sp",
        split_axis=0,
        concat_axis=0,
        tiled=True,
    )
    picked = returned.reshape(slot_total, model_width)[targets.reshape(-1)].astype(jnp.float32)
    picked = picked.reshape(route_rows, top_count, model_width)
    own_weights = lax.dynamic_slice_in_dim(route_weights, tp_here * route_rows, route_rows, 0)
    routed = jnp.sum(picked * own_weights[:, :, None], axis=1)
    return (own_rows.astype(jnp.float32) + routed).astype(jnp.bfloat16)


def local(*arrays):
    positions, top_count = arrays[11].shape
    shards = lax.axis_size("sp")
    route_rows = positions // lax.axis_size("tp")
    dense = shards == PLANE and 2 * top_count * route_rows // shards >= route_rows
    return (local_dense if dense else local_slotted)(*arrays)


def solution(mesh):
    return jax.shard_map(
        local,
        mesh=mesh,
        in_specs=(
            P("sp", "tp"),
            P("sp", "tp"),
            P("sp"),
            P(None, "tp"),
            P("tp", None, None),
            P("tp", None, None),
            P("tp"),
            P("tp"),
            P("tp", None),
            P("sp", None),
            P(),
            P("sp", None),
            P("sp", None),
            P("sp", None, "tp"),
            P("sp", None, "tp"),
            P("sp", "tp", None),
        ),
        out_specs=P(("sp", "tp"), None),
        check_vma=False,
    )
```

```python
import functools

import jax
import jax.numpy as jnp
from jax import lax
from jax.experimental import pallas as pl
from jax.experimental.pallas import tpu as pltpu
from jax.sharding import PartitionSpec as P

EPSILON = 1e-06
RATE_SCALE = 8.0
LANES = 128
SUBLANES = 8
CORES = 2
PLANE = 4


F32 = jnp.float32
BF16 = jnp.bfloat16


def vmem_call(kernel, outs, args, scratch=(), limit_mib=4, far_args=()):
    near, far = (pl.BlockSpec(memory_space=space) for space in (pltpu.VMEM, pltpu.HBM))
    return pl.pallas_call(
        kernel,
        in_specs=[far] * len(far_args) + [near] * len(args),
        out_specs=[near] * len(outs),
        out_shape=[jax.ShapeDtypeStruct(shape, dtype) for shape, dtype in outs],
        scratch_shapes=[
            pltpu.VMEM(*what) if isinstance(what, tuple) else what for what in scratch
        ],
        compiler_params=pltpu.CompilerParams(vmem_limit_bytes=limit_mib << 20),
    )(
        *[pltpu.with_memory_space_constraint(arg, pltpu.HBM) for arg in far_args],
        *[pltpu.with_memory_space_constraint(arg, pltpu.VMEM) for arg in args],
    )


def place():
    tp_here = lax.axis_index("tp")
    return lax.axis_index("sp"), tp_here // CORES, tp_here % CORES


def flip(value, axis, distance):
    return lax.ppermute(value, axis, [(i, i ^ distance) for i in range(lax.axis_size(axis))])


def flip_z(value, distance):
    return flip(value, "tp", distance * CORES)


def column(row):
    return jnp.transpose(jnp.broadcast_to(row, (LANES, row.shape[1])))


def one_minus_exp(value):
    series = jnp.ones_like(value)
    for order in range(7, 1, -1):
        series = 1.0 + value * series * (1.0 / order)
    return jnp.where(value > -0.35, -value * series, 1.0 - jnp.exp(value))


def scan_rows(decay, drive):
    rows = decay.shape[0]
    row_ids = lax.broadcasted_iota(jnp.int32, decay.shape, 0)
    distance = 1
    while distance < rows:
        if distance < SUBLANES:
            head = row_ids < distance
            earlier_decay = jnp.where(head, 1.0, pltpu.roll(decay, distance, 0))
            earlier_drive = jnp.where(head, 0.0, pltpu.roll(drive, distance, 0))
            drive = drive + decay * earlier_drive
            decay = decay * earlier_decay
        else:
            late_drive = drive[distance:] + decay[distance:] * drive[: rows - distance]
            late_decay = decay[distance:] * decay[: rows - distance]
            drive = jnp.concatenate([drive[:distance], late_drive], axis=0)
            decay = jnp.concatenate([decay[:distance], late_decay], axis=0)
        distance *= 2
    return decay, drive


def gated_terms(conv, starts, rate_w, inlet_w, decay_in):
    conv = conv.astype(BF16)
    rate = jax.nn.sigmoid(jnp.dot(conv, rate_w, preferred_element_type=F32))
    inlet = jax.nn.sigmoid(jnp.dot(conv, inlet_w, preferred_element_type=F32))
    negated = -decay_in
    soft = jnp.maximum(negated, 0.0) + jnp.log1p(jnp.exp(-jnp.abs(negated)))
    log_decay = -RATE_SCALE * rate * soft
    decay = jnp.where(starts, 0.0, jnp.exp(log_decay))
    norm = jnp.where(starts, 1.0, jnp.sqrt(one_minus_exp(2.0 * log_decay)))
    return decay, norm * inlet * conv.astype(F32)


def convolve(padded, docs, taps, at, count, lanes):
    reach = taps.shape[0] - 1
    own_doc = docs[at : at + count]
    conv = jnp.zeros((count, LANES), F32)
    for tap in range(reach + 1):
        source = slice(at - reach + tap, at - reach + tap + count)
        rows = padded[source, lanes]
        if tap < reach:
            rows = jnp.where(docs[source] == own_doc, rows, 0.0)
        conv = conv + rows * taps[tap : tap + 1, lanes].astype(F32)
    return conv, docs[at - 1 : at - 1 + count] != own_doc


EDGE = slice(SUBLANES, 2 * SUBLANES)
EDGE_DOCS = slice(2 * SUBLANES, 3 * SUBLANES)
MESSAGE_ROWS = 3 * SUBLANES


def lru_kernel(*refs):
    far, refs = refs[:13], refs[13:]
    (state_out, run_out, mix_out), refs = refs[:3], refs[3:]
    messages, refs = refs[:PLANE], refs[PLANE:]
    (taps, rate_w, inlet_w, decay_in, out_w, residual, down_w), refs = refs[:7], refs[7:]
    rows_in, gate_in, docs, gain, routes, route_w, padded, doc_cols, sems = refs
    block = residual.shape[0]
    own = pl.ds(pl.multiple_of(lax.axis_index("tp") * block, block), block)
    sources = [*far[:11], far[11].at[own], far[12]]
    targets = (
        rows_in, docs, taps, rate_w, inlet_w, decay_in, gate_in, gain, routes, route_w, out_w, residual,
        down_w,
    )
    copies = [
        pltpu.make_async_copy(source, target, sems.at[i])
        for i, (source, target) in enumerate(zip(sources, targets))
    ]
    for copy in copies:
        copy.start()
    for copy in copies[:-3]:
        copy.wait()
    positions, channels = rows_in.shape
    reach = taps.shape[0] - 1
    padded[0:SUBLANES] = jnp.zeros((SUBLANES, channels), F32)
    padded[SUBLANES:] = rows_in[...].astype(F32)
    doc_cols[0:SUBLANES] = jnp.zeros((SUBLANES, LANES), F32)
    doc_cols[SUBLANES:] = column(docs[...].astype(F32) + 1.0)
    later = lax.broadcasted_iota(jnp.int32, (positions, LANES), 0) >= reach
    for group in range(channels // LANES):
        lanes = slice(group * LANES, (group + 1) * LANES)
        conv, starts = convolve(padded, doc_cols, taps, SUBLANES, positions, lanes)
        decay, drive = gated_terms(
            conv, starts, rate_w[group], inlet_w[group], decay_in[0:1, lanes]
        )
        run, state = scan_rows(jnp.where(later, decay, 1.0), jnp.where(later, drive, 0.0))
        state_out[:, lanes] = state
        run_out[:, lanes] = run
        for message in messages:
            message[0:1, lanes] = run[positions - 1 :]
            message[1:2, lanes] = state[positions - 1 :]
        mix_out[:, lanes] = jax.nn.gelu(gate_in[:, lanes].astype(F32)) * gain[0:1, lanes]

    def ends(rows):
        begin, end = rows[SUBLANES : 2 * SUBLANES], rows[positions : positions + SUBLANES]
        row_ids = lax.broadcasted_iota(jnp.int32, begin.shape, 0)
        return jnp.where(row_ids < reach, begin, end)

    shard, _, _ = place()
    for k, message in enumerate(messages):
        dense = jnp.zeros((1, positions), F32)
        for choice in range(routes.shape[0]):
            chosen = routes[choice : choice + 1] == (shard ^ k)
            dense = dense + jnp.where(chosen, route_w[choice : choice + 1], 0.0)
        message[2:3, 0:positions] = dense
        message[EDGE, 0:channels] = ends(padded)
        message[EDGE_DOCS, 0:LANES] = ends(doc_cols)
    for copy in copies[-3:]:
        copy.wait()


def split_sum(total):
    lane_ids = lax.broadcasted_iota(jnp.int32, (total.shape[0], LANES), 1)
    high = total.astype(BF16).astype(F32)
    low = (total - high).astype(BF16).astype(F32)
    return jnp.where(lane_ids == 0, high, jnp.where(lane_ids == 1, low, 0.0)).astype(BF16)


def joined_sum(lanes):
    lanes = lanes.astype(F32)
    return lanes[:, 0:1] + lanes[:, 1:2]


def mix_kernel(state, run, mix, taps, rate_w, inlet_w, decay_in, *rest, block):
    *messages, keep, send, stacked, edge, edge_docs, terms, heads, hidden, mixed = rest
    channels = state.shape[1]
    reach = taps.shape[0] - 1
    for k, message in enumerate(messages):
        stacked[k] = message[...]
    shard, _, core = place()
    pair = 2 * SUBLANES
    for j in range(PLANE):
        here = stacked.at[j ^ shard]
        at = j * pair
        if j == 0:
            edge[at : at + SUBLANES] = jnp.zeros((SUBLANES, channels), F32)
            edge_docs[at : at + SUBLANES] = jnp.zeros((SUBLANES, LANES), F32)
        else:
            before = stacked.at[(j - 1) ^ shard]
            edge[at : at + SUBLANES] = before[EDGE, :channels]
            edge_docs[at : at + SUBLANES] = before[EDGE_DOCS, :LANES]
        edge[at + SUBLANES : at + pair] = here[EDGE, :channels]
        edge_docs[at + SUBLANES : at + pair] = here[EDGE_DOCS, :LANES]
    for group in range(channels // LANES):
        lanes = slice(group * LANES, (group + 1) * LANES)
        firsts = [
            convolve(edge, edge_docs, taps, j * pair + SUBLANES, SUBLANES, lanes)
            for j in range(PLANE)
        ]
        conv = jnp.concatenate([first[0] for first in firsts], axis=0)
        for j, (_, starts) in enumerate(firsts):
            rows = slice(j * SUBLANES, (j + 1) * SUBLANES)
            heads[j, :, lanes] = jnp.where(starts, 1.0, 0.0)
        starts = jnp.concatenate([heads[j, :, lanes] for j in range(PLANE)], axis=0) > 0.5
        terms[0, :, lanes], terms[1, :, lanes] = gated_terms(
            conv, starts, rate_w[group], inlet_w[group], decay_in[0:1, lanes]
        )
    carried = jnp.zeros((1, channels), F32)
    for j in range(PLANE):
        for row in range(reach):
            at = j * SUBLANES + row
            carried = terms[0, at : at + 1] * carried + terms[1, at : at + 1]
            heads[j, row : row + 1] = carried
        here = stacked.at[j ^ shard]
        carried = here[0:1, :channels] * carried + here[1:2, :channels]
    head = heads[shard]
    hidden[...] = state[...] + run[...] * head[reach - 1 : reach]
    early = lax.broadcasted_iota(jnp.int32, (SUBLANES, channels), 0) < reach
    hidden[0:SUBLANES] = jnp.where(early, head, hidden[0:SUBLANES])
    whole = hidden[...]
    mixed[:, :channels] = (whole * mix[...]).astype(BF16)
    mixed[:, channels:] = split_sum(jnp.sum(whole * whole, axis=1, keepdims=True))
    for z in range(keep.shape[0] // block):
        rows = slice(z * block, (z + 1) * block)
        keep[rows] = mixed[pl.ds(pl.multiple_of((CORES * z + core) * block, block), block)]
        send[rows] = mixed[pl.ds(pl.multiple_of((CORES * z + 1 - core) * block, block), block)]


def project_kernel(keep, other, own_w, other_w, *rest, block):
    *outs, own_rows, other_rows = rest
    channels, width = own_w.shape
    _, depth, _ = place()
    for k in range(len(outs)):
        rows = slice(k * block, (k + 1) * block)
        source = pl.ds(pl.multiple_of((depth ^ k) * block, block), block)
        own_rows[rows] = keep[source]
        other_rows[rows] = other[source]
    squares = split_sum(joined_sum(own_rows[:, channels:]) + joined_sum(other_rows[:, channels:]))
    product = jnp.dot(own_rows[:, :channels], own_w[...], preferred_element_type=F32)
    product = product + jnp.dot(other_rows[:, :channels], other_w[...], preferred_element_type=F32)
    for k, out in enumerate(outs):
        rows = slice(k * block, (k + 1) * block)
        out[:, :width] = product[rows].astype(BF16)
        out[:, width:] = squares[rows]


def norm_kernel(residual, gain, *rest, channels_total):
    *parts, after_out, normed_out = rest
    width = residual.shape[1]
    total = sum(part[:, :width].astype(F32) for part in parts)
    squares = sum(joined_sum(part[:, width:]) for part in parts)
    projected = total * lax.rsqrt(squares / channels_total + EPSILON)
    after = (residual[...].astype(F32) + projected).astype(BF16)
    after_out[...] = after
    floated = after.astype(F32)
    inverse_rms = lax.rsqrt(jnp.mean(floated * floated, axis=1, keepdims=True) + EPSILON)
    normed_out[...] = (floated * inverse_rms * gain[...]).astype(BF16)


def expert_kernel(*refs, labels, block, tile, out_tile):
    pieces, refs = refs[: len(labels)], refs[len(labels) :]
    messages, refs = refs[:PLANE], refs[PLANE:]
    (own_gate, other_gate, own_up, other_up, own_down, other_down), refs = refs[:6], refs[6:]
    outs, (tokens, weight_cols, weights, hidden) = refs[: len(labels)], refs[len(labels) :]
    half, width = own_down.shape
    positions = weight_cols.shape[1]
    _, depth, core = place()
    for k in range(PLANE):
        weight_cols[k] = column(messages[k][2:3, :positions])
    at = 0
    for piece, (z_flip, planes) in zip(pieces, labels):
        tokens[at : at + len(planes) * block] = piece[...]
        source = (CORES * (depth ^ z_flip) + core) * block
        for k in planes:
            weights[at : at + block] = weight_cols[k, pl.ds(pl.multiple_of(source, block), block)]
            at += block

    for base, gate_w, up_w in ((0, own_gate, own_up), (half, other_gate, other_up)):

        def hide(index, _):
            spot = pl.multiple_of(index * tile, LANES)
            gate = jnp.dot(tokens[...], gate_w[:, pl.ds(spot, tile)], preferred_element_type=F32)
            up = jnp.dot(tokens[...], up_w[:, pl.ds(spot, tile)], preferred_element_type=F32)
            spot = pl.multiple_of(base + spot, LANES)
            hidden[:, pl.ds(spot, tile)] = (jax.nn.silu(gate) * up).astype(BF16)
            return _

        lax.fori_loop(0, half // tile, hide, 0)

    def lower(index, _):
        cols = pl.ds(pl.multiple_of(index * out_tile, LANES), out_tile)
        product = jnp.dot(hidden[:, :half], own_down[:, cols], preferred_element_type=F32)
        product = product + jnp.dot(hidden[:, half:], other_down[:, cols], preferred_element_type=F32)
        scale = jnp.concatenate([weights[...]] * (out_tile // LANES), axis=1)
        scaled = (product * scale).astype(BF16)
        at = 0
        for out in outs:
            out[:, cols] = scaled[at : at + out.shape[0]]
            at += out.shape[0]
        return _

    lax.fori_loop(0, width // out_tile, lower, 0)


def run_experts(pieces, labels, messages, weights, block):
    half, width = weights[-1].shape
    rows = sum(piece.shape[0] for piece in pieces)
    positions = block * lax.axis_size("tp")
    return vmem_call(
        functools.partial(
            expert_kernel, labels=labels, block=block, tile=half, out_tile=width // 2
        ),
        [(piece.shape, BF16) for piece in pieces],
        [*pieces, *messages, *weights],
        scratch=[
            ((rows, width), BF16),
            ((PLANE, positions, LANES), F32),
            ((rows, LANES), F32),
            ((rows, 2 * half), BF16),
        ],
        limit_mib=10,
    )


def spread_direct(rows, _):
    pieces = [rows] + [flip(rows, "sp", k) for k in range(1, PLANE)]
    return pieces, [(k,) for k in range(PLANE)]


def reduce_direct(outs, _):
    parts = [outs[0]] + [flip(outs[k], "sp", k) for k in range(1, PLANE)]
    return sum(part.astype(F32) for part in parts).astype(BF16)


def plane_order(z_flip):
    return (1, 2) if z_flip % 2 == 0 else (2, 1)


def spread_staged(rows, z_flip):
    near, far = plane_order(z_flip)
    pair = jnp.concatenate([rows, flip(rows, "sp", near)], axis=0)
    return [pair, flip(pair, "sp", far)], [(0, near), (far, near | far)]


def reduce_staged(outs, z_flip):
    near, far = plane_order(z_flip)
    block = outs[0].shape[0] // 2
    summed = (outs[0].astype(F32) + flip(outs[1], "sp", far).astype(F32)).astype(BF16)
    return (summed[:block].astype(F32) + flip(summed[block:], "sp", near).astype(F32)).astype(BF16)


def local_dense(
    lru_input, gate_input, documents, conv_taps, rate_weight, inlet_weight, decay_param, lru_gain,
    out_weight, residual, ffn_gain, routes, route_weights, w_gate, w_up, w_down,
):
    positions, channels = lru_input.shape
    width = residual.shape[1]
    tp_count = lax.axis_size("tp")
    depths = tp_count // CORES
    block = positions // tp_count
    span = max(positions, channels)

    other_out = flip(out_weight, "tp", 1)

    state, run, mix, *rest = vmem_call(
        lru_kernel,
        [((positions, channels), F32)] * 3
        + [((MESSAGE_ROWS, span), F32)] * PLANE
        + [
            (conv_taps.shape, BF16), (rate_weight.shape, BF16), (inlet_weight.shape, BF16),
            ((1, channels), F32), (out_weight.shape, BF16), ((block, width), BF16),
            (w_down.shape[1:], BF16),
        ],
        [],
        scratch=[
            ((positions, channels), BF16),
            ((positions, channels), BF16),
            ((1, positions), jnp.int32),
            ((1, channels), F32),
            (routes.T.shape, jnp.int32),
            (routes.T.shape, F32),
            ((SUBLANES + positions, channels), F32),
            ((SUBLANES + positions, LANES), F32),
            pltpu.SemaphoreType.DMA((13,)),
        ],
        far_args=[
            lru_input, documents[None, :], conv_taps, rate_weight, inlet_weight,
            decay_param[None, :], gate_input, lru_gain[None, :], routes.T, route_weights.T,
            out_weight, residual, w_down[0],
        ],
    )
    messages, params = rest[:PLANE], rest[PLANE:]
    taps, rate_w, inlet_w, decay_in, own_out, own_residual, own_down = params
    messages = [messages[0]] + [flip(messages[k], "sp", k) for k in range(1, PLANE)]
    messages, other_out = lax.optimization_barrier((messages, other_out))

    half_rows = positions // CORES
    packed = (half_rows, channels + LANES)
    keep, send = vmem_call(
        functools.partial(mix_kernel, block=block),
        [(packed, BF16)] * 2,
        [state, run, mix, taps, rate_w, inlet_w, decay_in, *messages],
        scratch=[
            ((PLANE, MESSAGE_ROWS, span), F32),
            ((2 * PLANE * SUBLANES, channels), F32),
            ((2 * PLANE * SUBLANES, LANES), F32),
            ((2, PLANE * SUBLANES, channels), F32),
            ((PLANE, SUBLANES, channels), F32),
            ((positions, channels), F32),
            ((positions, channels + LANES), BF16),
        ],
    )
    other, *own = lax.optimization_barrier((flip(send, "tp", 1), w_gate[0], w_up[0], w_down[0]))
    swapped = [flip(value, "tp", 1) for value in own]
    parts = vmem_call(
        functools.partial(project_kernel, block=block),
        [((block, width + LANES), BF16)] * depths,
        [keep, other, own_out, other_out],
        scratch=[(packed, BF16)] * 2,
    )
    parts = [parts[0]] + [flip_z(parts[k], k) for k in range(1, depths)]
    after, normed = vmem_call(
        functools.partial(norm_kernel, channels_total=channels * tp_count),
        [((block, width), BF16)] * 2,
        [own_residual, ffn_gain[None, :], *parts],
    )

    weights = (w_gate[0], swapped[0], w_up[0], swapped[1], own_down, swapped[2])
    rows_at = [normed] + [flip_z(normed, k) for k in range(1, depths)]
    near_flips, far_flips = tuple(range(min(2, depths))), range(2, depths)
    finished = {}
    for z_flips, direct in [((k,), True) for k in far_flips] + [(near_flips, False)]:
        spread = spread_direct if direct else spread_staged
        gathered = [spread(rows_at[k], k) for k in z_flips]
        pieces = [piece for some, _ in gathered for piece in some]
        labels = [(k, planes) for k, (_, some) in zip(z_flips, gathered) for planes in some]
        outs = run_experts(pieces, tuple(labels), messages, weights, block)
        for k in z_flips:
            count = len(outs) // len(z_flips)
            own_outs = outs[z_flips.index(k) * count :][:count]
            finished[k] = (reduce_direct if direct else reduce_staged)(own_outs, k)
    total = after.astype(F32) + finished[0].astype(F32)
    for k in range(1, depths):
        total = total + flip_z(finished[k], k).astype(F32)
    return total.astype(BF16)


def shifted(block, axis, distance):
    devices = range(lax.axis_size(axis))
    route = [(i - distance, i) for i in devices if i - distance in devices]
    return lax.ppermute(block, axis, route)


def carried_in(value, axis, join, neutral):
    count, mine = (lax.axis_size(axis), lax.axis_index(axis))
    pieces = jax.tree.map(lambda part: lax.all_gather(part, axis), value)
    so_far = jax.tree.map(
        lambda part, zero: jnp.full_like(part, 0) + jnp.asarray(zero, part.dtype), value, neutral
    )

    def hop(position, so_far):
        longer = join(so_far, jax.tree.map(lambda part: part[position], pieces))
        return jax.tree.map(lambda new, old: jnp.where(position < mine, new, old), longer, so_far)

    return lax.fori_loop(0, count - 1, hop, so_far)


def join_runs(earlier_run, later_run):
    return (earlier_run[0] * later_run[0], later_run[0] * earlier_run[1] + later_run[1])


def slot_targets(route_block, expert_count, capacity):
    flat_routes = route_block.reshape(-1)
    onehot = (flat_routes[:, None] == jnp.arange(expert_count, dtype=jnp.int32)[None, :]).astype(
        jnp.int32
    )
    earlier_hits = jnp.cumsum(onehot, axis=0) - onehot
    slot_index = jnp.sum(earlier_hits * onehot, axis=1)
    return (flat_routes * capacity + slot_index).reshape(route_block.shape)


def pick_matrix(targets, slot_total):
    slot_hits = targets[None, :, :] == jnp.arange(slot_total, dtype=jnp.int32)[:, None, None]
    return jnp.sum(slot_hits.astype(jnp.int32), axis=2).astype(jnp.bfloat16)


def rms_rows(row_block, gain_vector):
    floated = row_block.astype(jnp.float32)
    inverse_rms = lax.rsqrt(jnp.mean(floated * floated, axis=1, keepdims=True) + EPSILON)
    return (floated * inverse_rms * gain_vector[None, :]).astype(jnp.bfloat16)


def expert_apply(row_piece, gate_weight, up_weight, down_weight):
    gate_part = jnp.dot(row_piece, gate_weight, preferred_element_type=jnp.float32)
    up_part = jnp.dot(row_piece, up_weight, preferred_element_type=jnp.float32)
    hidden_units = (jax.nn.silu(gate_part) * up_part).astype(jnp.bfloat16)
    return jnp.dot(hidden_units, down_weight, preferred_element_type=jnp.float32)


def local_slotted(
    lru_input,
    gate_input,
    documents,
    conv_taps,
    rate_weight,
    inlet_weight,
    decay_param,
    lru_gain,
    out_weight,
    residual,
    ffn_gain,
    routes,
    route_weights,
    w_gate,
    w_up,
    w_down,
):
    positions = lru_input.shape[0]
    channels = lru_input.shape[1]
    model_width = residual.shape[1]
    reach_back = conv_taps.shape[0] - 1
    tail_rows, tail_docs = shifted(
        (lru_input[positions - reach_back :], documents[positions - reach_back :] + 1), "sp", 1
    )
    prior_docs = jnp.concatenate([tail_docs - 1, documents])
    padded_input = jnp.concatenate([tail_rows, lru_input], axis=0)
    conv_sum = jnp.zeros((positions, channels), jnp.float32)
    for tap_index in range(reach_back + 1):
        same_doc = (prior_docs[tap_index : tap_index + positions] == documents).astype(jnp.float32)[
            :, None
        ]
        conv_sum = (
            conv_sum
            + padded_input[tap_index : tap_index + positions].astype(jnp.float32)
            * conv_taps[tap_index].astype(jnp.float32)[None, :]
            * same_doc
        )
    convolved = conv_sum.astype(jnp.bfloat16)
    grouped = convolved.reshape(positions, rate_weight.shape[0], rate_weight.shape[1])
    rate_gate = jax.nn.sigmoid(
        jnp.einsum(
            "tnc,ncd->tnd", grouped, rate_weight, preferred_element_type=jnp.float32
        ).reshape(positions, channels)
    )
    inlet_gate = jax.nn.sigmoid(
        jnp.einsum(
            "tnc,ncd->tnd", grouped, inlet_weight, preferred_element_type=jnp.float32
        ).reshape(positions, channels)
    )
    log_decay = -RATE_SCALE * rate_gate * jax.nn.softplus(-decay_param)[None, :]
    starts = (prior_docs[reach_back - 1 : reach_back - 1 + positions] != documents)[:, None]
    decay_step = jnp.where(starts, 0.0, jnp.exp(log_decay))
    norm_factor = jnp.where(starts, 1.0, jnp.sqrt(-jnp.expm1(2.0 * log_decay)))
    drive_term = norm_factor * inlet_gate * convolved.astype(jnp.float32)
    decay_run, local_state = lax.associative_scan(join_runs, (decay_step, drive_term), axis=0)
    carried = carried_in(
        (decay_run[positions - 1], local_state[positions - 1]),
        "sp",
        join_runs,
        (jnp.ones((channels,), jnp.float32), jnp.zeros((channels,), jnp.float32)),
    )
    hidden_state = local_state + decay_run * carried[1][None, :]
    square_sums = lax.psum(jnp.sum(hidden_state * hidden_state, axis=1), "tp")
    inverse_rms = lax.rsqrt(square_sums[:, None] / (channels * lax.axis_size("tp")) + EPSILON)
    mixer_rows = (
        hidden_state * inverse_rms * lru_gain[None, :] * jax.nn.gelu(gate_input.astype(jnp.float32))
    ).astype(jnp.bfloat16)
    tp_count = lax.axis_size("tp")
    tp_here = lax.axis_index("tp")
    expert_count = lax.axis_size("sp")
    route_rows = positions // tp_count
    top_count = routes.shape[1]
    capacity = 2 * top_count * route_rows // expert_count
    slot_total = expert_count * capacity
    projected = lax.psum_scatter(
        jnp.dot(mixer_rows, out_weight, preferred_element_type=jnp.float32).astype(jnp.bfloat16),
        "tp",
        scatter_dimension=0,
        tiled=True,
    ).astype(jnp.float32)
    own_rows = (
        lax.dynamic_slice_in_dim(residual, tp_here * route_rows, route_rows, 0).astype(jnp.float32)
        + projected
    ).astype(jnp.bfloat16)
    own_routes = lax.dynamic_slice_in_dim(routes, tp_here * route_rows, route_rows, 0)
    targets = slot_targets(own_routes, expert_count, capacity)
    outgoing = jnp.dot(
        pick_matrix(targets, slot_total),
        rms_rows(own_rows, ffn_gain),
        preferred_element_type=jnp.float32,
    ).astype(jnp.bfloat16)
    arrived = lax.all_to_all(
        outgoing.reshape(expert_count, capacity, model_width),
        "sp",
        split_axis=0,
        concat_axis=0,
        tiled=True,
    )
    partial_out = expert_apply(
        lax.all_gather(arrived.reshape(slot_total, model_width), "tp", axis=0, tiled=True),
        w_gate[0],
        w_up[0],
        w_down[0],
    )
    expert_out = lax.psum_scatter(
        partial_out.astype(jnp.bfloat16), "tp", scatter_dimension=0, tiled=True
    )
    returned = lax.all_to_all(
        expert_out.reshape(expert_count, capacity, model_width),
        "sp",
        split_axis=0,
        concat_axis=0,
        tiled=True,
    )
    picked = returned.reshape(slot_total, model_width)[targets.reshape(-1)].astype(jnp.float32)
    picked = picked.reshape(route_rows, top_count, model_width)
    own_weights = lax.dynamic_slice_in_dim(route_weights, tp_here * route_rows, route_rows, 0)
    routed = jnp.sum(picked * own_weights[:, :, None], axis=1)
    return (own_rows.astype(jnp.float32) + routed).astype(jnp.bfloat16)


def local(*arrays):
    positions, top_count = arrays[11].shape
    shards = lax.axis_size("sp")
    route_rows = positions // lax.axis_size("tp")
    dense = shards == PLANE and 2 * top_count * route_rows // shards >= route_rows
    return (local_dense if dense else local_slotted)(*arrays)


def solution(mesh):
    return jax.shard_map(
        local,
        mesh=mesh,
        in_specs=(
            P("sp", "tp"),
            P("sp", "tp"),
            P("sp"),
            P(None, "tp"),
            P("tp", None, None),
            P("tp", None, None),
            P("tp"),
            P("tp"),
            P("tp", None),
            P("sp", None),
            P(),
            P("sp", None),
            P("sp", None),
            P("sp", None, "tp"),
            P("sp", None, "tp"),
            P("sp", "tp", None),
        ),
        out_specs=P(("sp", "tp"), None),
        check_vma=False,
    )
```

```python
import functools

import jax
import jax.numpy as jnp
from jax import lax
from jax.experimental import pallas as pl
from jax.experimental.pallas import tpu as pltpu
from jax.sharding import PartitionSpec as P


EPSILON = 1e-06
RATE_SCALE = 8.0
LANES = 128
SUBLANES = 8
CORES = 2
PLANE = 4


F32 = jnp.float32
BF16 = jnp.bfloat16


def vmem_call(kernel, outs, args, scratch=(), limit_mib=4, far_args=()):
    near, far = (pl.BlockSpec(memory_space=space) for space in (pltpu.VMEM, pltpu.HBM))
    return pl.pallas_call(
        kernel,
        in_specs=[far] * len(far_args) + [near] * len(args),
        out_specs=[near] * len(outs),
        out_shape=[jax.ShapeDtypeStruct(shape, dtype) for shape, dtype in outs],
        scratch_shapes=[
            pltpu.VMEM(*what) if isinstance(what, tuple) else what for what in scratch
        ],
        compiler_params=pltpu.CompilerParams(vmem_limit_bytes=limit_mib << 20),
    )(
        *[pltpu.with_memory_space_constraint(arg, pltpu.HBM) for arg in far_args],
        *[pltpu.with_memory_space_constraint(arg, pltpu.VMEM) for arg in args],
    )


def place():
    tp_here = lax.axis_index("tp")
    return lax.axis_index("sp"), tp_here // CORES, tp_here % CORES


def flip(value, axis, distance):
    return lax.ppermute(value, axis, [(i, i ^ distance) for i in range(lax.axis_size(axis))])


def flip_plane(value, order):
    tp_count = lax.axis_size("tp")
    pairs = [
        (shard * tp_count + at, (shard ^ plane_flip(at % CORES, order)) * tp_count + at)
        for shard in range(PLANE)
        for at in range(tp_count)
    ]
    return lax.ppermute(value, ("sp", "tp"), pairs)


def plane_flip(core, order):
    return 1 + core if order == 0 else 2 - core


def flip_z(value, distance):
    return flip(value, "tp", distance * CORES)


def column(row):
    return jnp.transpose(jnp.broadcast_to(row, (LANES, row.shape[1])))


def one_minus_exp(value):
    series = jnp.ones_like(value)
    for order in range(7, 1, -1):
        series = 1.0 + value * series * (1.0 / order)
    return jnp.where(value > -0.35, -value * series, 1.0 - jnp.exp(value))


def scan_rows(decay, drive):
    rows = decay.shape[0]
    row_ids = lax.broadcasted_iota(jnp.int32, decay.shape, 0)
    distance = 1
    while distance < rows:
        if distance < SUBLANES:
            head = row_ids < distance
            earlier_decay = jnp.where(head, 1.0, pltpu.roll(decay, distance, 0))
            earlier_drive = jnp.where(head, 0.0, pltpu.roll(drive, distance, 0))
            drive = drive + decay * earlier_drive
            decay = decay * earlier_decay
        else:
            late_drive = drive[distance:] + decay[distance:] * drive[: rows - distance]
            late_decay = decay[distance:] * decay[: rows - distance]
            drive = jnp.concatenate([drive[:distance], late_drive], axis=0)
            decay = jnp.concatenate([decay[:distance], late_decay], axis=0)
        distance *= 2
    return decay, drive


def gated_terms(conv, starts, rate_w, inlet_w, decay_in):
    conv = conv.astype(BF16)
    rate = jax.nn.sigmoid(jnp.dot(conv, rate_w, preferred_element_type=F32))
    inlet = jax.nn.sigmoid(jnp.dot(conv, inlet_w, preferred_element_type=F32))
    negated = -decay_in
    soft = jnp.maximum(negated, 0.0) + jnp.log1p(jnp.exp(-jnp.abs(negated)))
    log_decay = -RATE_SCALE * rate * soft
    decay = jnp.where(starts, 0.0, jnp.exp(log_decay))
    norm = jnp.where(starts, 1.0, jnp.sqrt(one_minus_exp(2.0 * log_decay)))
    return decay, norm * inlet * conv.astype(F32)


def convolve(padded, docs, taps, at, count, lanes):
    reach = taps.shape[0] - 1
    own_doc = docs[at : at + count]
    conv = jnp.zeros((count, LANES), F32)
    for tap in range(reach + 1):
        source = slice(at - reach + tap, at - reach + tap + count)
        rows = padded[source, lanes]
        if tap < reach:
            rows = jnp.where(docs[source] == own_doc, rows, 0.0)
        conv = conv + rows * taps[tap : tap + 1, lanes].astype(F32)
    return conv, docs[at - 1 : at - 1 + count] != own_doc


EDGE = slice(SUBLANES, 2 * SUBLANES)
EDGE_DOCS = slice(2 * SUBLANES, 3 * SUBLANES)
MESSAGE_ROWS = 3 * SUBLANES


def lru_kernel(*refs):
    far, refs = refs[:13], refs[13:]
    (state_out, run_out, mix_out), refs = refs[:3], refs[3:]
    messages, refs = refs[:PLANE], refs[PLANE:]
    (taps, rate_w, inlet_w, decay_in, out_w, residual, down_w), refs = refs[:7], refs[7:]
    rows_in, gate_in, docs, gain, routes, route_w, padded, doc_cols, sems = refs
    block = residual.shape[0]
    own = pl.ds(pl.multiple_of(lax.axis_index("tp") * block, block), block)
    sources = [*far[:11], far[11].at[own], far[12]]
    targets = (
        rows_in, docs, taps, rate_w, inlet_w, decay_in, gate_in, gain, routes, route_w, out_w, residual,
        down_w,
    )
    copies = [
        pltpu.make_async_copy(source, target, sems.at[i])
        for i, (source, target) in enumerate(zip(sources, targets))
    ]
    for copy in copies:
        copy.start()
    for copy in copies[:-3]:
        copy.wait()
    positions, channels = rows_in.shape
    reach = taps.shape[0] - 1
    padded[0:SUBLANES] = jnp.zeros((SUBLANES, channels), F32)
    padded[SUBLANES:] = rows_in[...].astype(F32)
    doc_cols[0:SUBLANES] = jnp.zeros((SUBLANES, LANES), F32)
    doc_cols[SUBLANES:] = column(docs[...].astype(F32) + 1.0)
    later = lax.broadcasted_iota(jnp.int32, (positions, LANES), 0) >= reach
    for group in range(channels // LANES):
        lanes = slice(group * LANES, (group + 1) * LANES)
        conv, starts = convolve(padded, doc_cols, taps, SUBLANES, positions, lanes)
        decay, drive = gated_terms(
            conv, starts, rate_w[group], inlet_w[group], decay_in[0:1, lanes]
        )
        run, state = scan_rows(jnp.where(later, decay, 1.0), jnp.where(later, drive, 0.0))
        state_out[:, lanes] = state
        run_out[:, lanes] = run
        for message in messages:
            message[0:1, lanes] = run[positions - 1 :]
            message[1:2, lanes] = state[positions - 1 :]
        mix_out[:, lanes] = jax.nn.gelu(gate_in[:, lanes].astype(F32)) * gain[0:1, lanes]

    def ends(rows):
        begin, end = rows[SUBLANES : 2 * SUBLANES], rows[positions : positions + SUBLANES]
        row_ids = lax.broadcasted_iota(jnp.int32, begin.shape, 0)
        return jnp.where(row_ids < reach, begin, end)

    shard, _, _ = place()
    for k, message in enumerate(messages):
        dense = jnp.zeros((1, positions), F32)
        for choice in range(routes.shape[0]):
            chosen = routes[choice : choice + 1] == (shard ^ k)
            dense = dense + jnp.where(chosen, route_w[choice : choice + 1], 0.0)
        message[2:3, 0:positions] = dense
        message[EDGE, 0:channels] = ends(padded)
        message[EDGE_DOCS, 0:LANES] = ends(doc_cols)
    for copy in copies[-3:]:
        copy.wait()


def split_sum(total):
    lane_ids = lax.broadcasted_iota(jnp.int32, (total.shape[0], LANES), 1)
    high = total.astype(BF16).astype(F32)
    low = (total - high).astype(BF16).astype(F32)
    return jnp.where(lane_ids == 0, high, jnp.where(lane_ids == 1, low, 0.0)).astype(BF16)


def joined_sum(lanes):
    lanes = lanes.astype(F32)
    return lanes[:, 0:1] + lanes[:, 1:2]


def mix_kernel(state, run, mix, taps, rate_w, inlet_w, decay_in, *rest, block):
    *messages, keep, send, stacked, edge, edge_docs, terms, heads, hidden, mixed = rest
    channels = state.shape[1]
    reach = taps.shape[0] - 1
    for k, message in enumerate(messages):
        stacked[k] = message[...]
    shard, _, core = place()
    pair = 2 * SUBLANES
    for j in range(PLANE):
        here = stacked.at[j ^ shard]
        at = j * pair
        if j == 0:
            edge[at : at + SUBLANES] = jnp.zeros((SUBLANES, channels), F32)
            edge_docs[at : at + SUBLANES] = jnp.zeros((SUBLANES, LANES), F32)
        else:
            before = stacked.at[(j - 1) ^ shard]
            edge[at : at + SUBLANES] = before[EDGE, :channels]
            edge_docs[at : at + SUBLANES] = before[EDGE_DOCS, :LANES]
        edge[at + SUBLANES : at + pair] = here[EDGE, :channels]
        edge_docs[at + SUBLANES : at + pair] = here[EDGE_DOCS, :LANES]
    for group in range(channels // LANES):
        lanes = slice(group * LANES, (group + 1) * LANES)
        firsts = [
            convolve(edge, edge_docs, taps, j * pair + SUBLANES, SUBLANES, lanes)
            for j in range(PLANE)
        ]
        conv = jnp.concatenate([first[0] for first in firsts], axis=0)
        for j, (_, starts) in enumerate(firsts):
            rows = slice(j * SUBLANES, (j + 1) * SUBLANES)
            heads[j, :, lanes] = jnp.where(starts, 1.0, 0.0)
        starts = jnp.concatenate([heads[j, :, lanes] for j in range(PLANE)], axis=0) > 0.5
        terms[0, :, lanes], terms[1, :, lanes] = gated_terms(
            conv, starts, rate_w[group], inlet_w[group], decay_in[0:1, lanes]
        )
    carried = jnp.zeros((1, channels), F32)
    for j in range(PLANE):
        for row in range(reach):
            at = j * SUBLANES + row
            carried = terms[0, at : at + 1] * carried + terms[1, at : at + 1]
            heads[j, row : row + 1] = carried
        here = stacked.at[j ^ shard]
        carried = here[0:1, :channels] * carried + here[1:2, :channels]
    head = heads[shard]
    hidden[...] = state[...] + run[...] * head[reach - 1 : reach]
    early = lax.broadcasted_iota(jnp.int32, (SUBLANES, channels), 0) < reach
    hidden[0:SUBLANES] = jnp.where(early, head, hidden[0:SUBLANES])
    whole = hidden[...]
    mixed[:, :channels] = (whole * mix[...]).astype(BF16)
    mixed[:, channels:] = split_sum(jnp.sum(whole * whole, axis=1, keepdims=True))
    for z in range(keep.shape[0] // block):
        rows = slice(z * block, (z + 1) * block)
        keep[rows] = mixed[pl.ds(pl.multiple_of((CORES * z + core) * block, block), block)]
        send[rows] = mixed[pl.ds(pl.multiple_of((CORES * z + 1 - core) * block, block), block)]


def project_kernel(keep, other, own_w, other_w, *rest, block):
    *outs, own_rows, other_rows = rest
    channels, width = own_w.shape
    _, depth, _ = place()
    for k in range(len(outs)):
        rows = slice(k * block, (k + 1) * block)
        source = pl.ds(pl.multiple_of((depth ^ k) * block, block), block)
        own_rows[rows] = keep[source]
        other_rows[rows] = other[source]
    squares = split_sum(joined_sum(own_rows[:, channels:]) + joined_sum(other_rows[:, channels:]))
    product = jnp.dot(own_rows[:, :channels], own_w[...], preferred_element_type=F32)
    product = product + jnp.dot(other_rows[:, :channels], other_w[...], preferred_element_type=F32)
    for k, out in enumerate(outs):
        rows = slice(k * block, (k + 1) * block)
        out[:, :width] = product[rows].astype(BF16)
        out[:, width:] = squares[rows]


def add_kernel(one, two, out):
    width = out.shape[1] - LANES
    out[:, :width] = (one[:, :width].astype(F32) + two[:, :width].astype(F32)).astype(BF16)
    out[:, width:] = split_sum(joined_sum(one[:, width:]) + joined_sum(two[:, width:]))


def norm_kernel(residual, gain, *rest, channels_total):
    *parts, after_out, normed_out = rest
    width = residual.shape[1]
    total = sum(part[:, :width].astype(F32) for part in parts)
    squares = sum(joined_sum(part[:, width:]) for part in parts)
    projected = total * lax.rsqrt(squares / channels_total + EPSILON)
    after = (residual[...].astype(F32) + projected).astype(BF16)
    after_out[...] = after
    floated = after.astype(F32)
    inverse_rms = lax.rsqrt(jnp.mean(floated * floated, axis=1, keepdims=True) + EPSILON)
    normed_out[...] = (floated * inverse_rms * gain[...]).astype(BF16)


def expert_kernel(*refs, z_flips, block, tile, out_tile):
    pieces, refs = refs[:2], refs[2:]
    messages, refs = refs[:PLANE], refs[PLANE:]
    (own_gate, other_gate, own_up, other_up, own_down, other_down), refs = refs[:6], refs[6:]
    outs, (tokens, weight_cols, weights, hidden) = refs[:2], refs[2:]
    half, width = own_down.shape
    positions = weight_cols.shape[1]
    _, depth, core = place()
    for k in range(PLANE):
        weight_cols[k] = column(messages[k][2:3, :positions])
    planes = ((0, plane_flip(core, 0)), (plane_flip(core, 1), PLANE - 1))
    at = 0
    for piece, halves in zip(pieces, planes):
        tokens[at : at + piece.shape[0]] = piece[...]
        for k in halves:
            for z_flip in z_flips:
                source = pl.multiple_of((CORES * (depth ^ z_flip) + core) * block, block)
                weights[at : at + block] = weight_cols[k, pl.ds(source, block)]
                at += block

    for base, gate_w, up_w in ((0, own_gate, own_up), (half, other_gate, other_up)):

        def hide(index, _):
            spot = pl.multiple_of(index * tile, LANES)
            gate = jnp.dot(tokens[...], gate_w[:, pl.ds(spot, tile)], preferred_element_type=F32)
            up = jnp.dot(tokens[...], up_w[:, pl.ds(spot, tile)], preferred_element_type=F32)
            spot = pl.multiple_of(base + spot, LANES)
            hidden[:, pl.ds(spot, tile)] = (jax.nn.silu(gate) * up).astype(BF16)
            return _

        lax.fori_loop(0, half // tile, hide, 0)

    def lower(index, _):
        cols = pl.ds(pl.multiple_of(index * out_tile, LANES), out_tile)
        product = jnp.dot(hidden[:, :half], own_down[:, cols], preferred_element_type=F32)
        product = product + jnp.dot(hidden[:, half:], other_down[:, cols], preferred_element_type=F32)
        scale = jnp.concatenate([weights[...]] * (out_tile // LANES), axis=1)
        scaled = (product * scale).astype(BF16)
        at = 0
        for out in outs:
            out[:, cols] = scaled[at : at + out.shape[0]]
            at += out.shape[0]
        return _

    lax.fori_loop(0, width // out_tile, lower, 0)


def run_experts(pieces, z_flips, messages, weights, block):
    half, width = weights[-1].shape
    rows = sum(piece.shape[0] for piece in pieces)
    positions = block * lax.axis_size("tp")
    return vmem_call(
        functools.partial(
            expert_kernel, z_flips=z_flips, block=block, tile=half, out_tile=width // 2
        ),
        [(piece.shape, BF16) for piece in pieces],
        [*pieces, *messages, *weights],
        scratch=[
            ((rows, width), BF16),
            ((PLANE, positions, LANES), F32),
            ((rows, LANES), F32),
            ((rows, 2 * half), BF16),
        ],
        limit_mib=10,
    )


def float_sum(parts):
    return sum(part.astype(F32) for part in parts)


def spread(rows):
    near = flip_plane(rows, 0)
    pair = jnp.concatenate([rows, near])
    return [pair, flip_plane(pair, 1)]


def gather_sum(outs):
    half = outs[0].shape[0] // 2
    far = flip_plane(outs[1], 1)
    near = float_sum([outs[0][half:], far[half:]]).astype(BF16)
    near = flip_plane(near, 0)
    return float_sum([outs[0][:half], far[:half], near]).astype(BF16)


def local_dense(
    lru_input, gate_input, documents, conv_taps, rate_weight, inlet_weight, decay_param, lru_gain,
    out_weight, residual, ffn_gain, routes, route_weights, w_gate, w_up, w_down,
):
    positions, channels = lru_input.shape
    width = residual.shape[1]
    tp_count = lax.axis_size("tp")
    depths = tp_count // CORES
    block = positions // tp_count
    span = max(positions, channels)

    other_out = flip(out_weight, "tp", 1)

    state, run, mix, *rest = vmem_call(
        lru_kernel,
        [((positions, channels), F32)] * 3
        + [((MESSAGE_ROWS, span), F32)] * PLANE
        + [
            (conv_taps.shape, BF16), (rate_weight.shape, BF16), (inlet_weight.shape, BF16),
            ((1, channels), F32), (out_weight.shape, BF16), ((block, width), BF16),
            (w_down.shape[1:], BF16),
        ],
        [],
        scratch=[
            ((positions, channels), BF16),
            ((positions, channels), BF16),
            ((1, positions), jnp.int32),
            ((1, channels), F32),
            (routes.T.shape, jnp.int32),
            (routes.T.shape, F32),
            ((SUBLANES + positions, channels), F32),
            ((SUBLANES + positions, LANES), F32),
            pltpu.SemaphoreType.DMA((13,)),
        ],
        far_args=[
            lru_input, documents[None, :], conv_taps, rate_weight, inlet_weight,
            decay_param[None, :], gate_input, lru_gain[None, :], routes.T, route_weights.T,
            out_weight, residual, w_down[0],
        ],
    )
    messages, params = rest[:PLANE], rest[PLANE:]
    taps, rate_w, inlet_w, decay_in, own_out, own_residual, own_down = params
    messages = [messages[0]] + [flip(messages[k], "sp", k) for k in range(1, PLANE)]
    early = flip(w_gate[0], "tp", 1)
    messages, other_out, early = lax.optimization_barrier((messages, other_out, early))

    half_rows = positions // CORES
    packed = (half_rows, channels + LANES)
    keep, send = vmem_call(
        functools.partial(mix_kernel, block=block),
        [(packed, BF16)] * 2,
        [state, run, mix, taps, rate_w, inlet_w, decay_in, *messages],
        scratch=[
            ((PLANE, MESSAGE_ROWS, span), F32),
            ((2 * PLANE * SUBLANES, channels), F32),
            ((2 * PLANE * SUBLANES, LANES), F32),
            ((2, PLANE * SUBLANES, channels), F32),
            ((PLANE, SUBLANES, channels), F32),
            ((positions, channels), F32),
            ((positions, channels + LANES), BF16),
        ],
    )
    other, *own = lax.optimization_barrier((flip(send, "tp", 1), w_up[0], w_down[0]))
    swapped = [early] + [flip(value, "tp", 1) for value in own]
    parts = vmem_call(
        functools.partial(project_kernel, block=block),
        [((block, width + LANES), BF16)] * depths,
        [keep, other, own_out, other_out],
        scratch=[(packed, BF16)] * 2,
    )
    parts = dict(enumerate(parts))
    for k in range(depths - 1, 1, -1):
        relay = k & -k
        if relay != k:
            passed = flip_z(parts.pop(k), relay)
            [parts[k ^ relay]] = vmem_call(
                add_kernel, [((block, width + LANES), BF16)], [parts[k ^ relay], passed]
            )
    parts = [parts[k] if k == 0 else flip_z(parts[k], k) for k in parts]
    after, normed = vmem_call(
        functools.partial(norm_kernel, channels_total=channels * tp_count),
        [((block, width), BF16)] * 2,
        [own_residual, ffn_gain[None, :], *parts],
    )

    weights = (w_gate[0], swapped[0], w_up[0], swapped[1], own_down, swapped[2])
    rows_at = [normed] + [flip_z(normed, k) for k in range(1, depths)]
    total = after.astype(F32)
    for k in range(depths):
        pieces = spread(rows_at[k])
        outs = run_experts(pieces, (k,), messages, weights, block)
        summed = gather_sum(outs)
        total = total + (flip_z(summed, k) if k else summed).astype(F32)
    return total.astype(BF16)


def shifted(block, axis, distance):
    devices = range(lax.axis_size(axis))
    route = [(i - distance, i) for i in devices if i - distance in devices]
    return lax.ppermute(block, axis, route)


def carried_in(value, axis, join, neutral):
    count, mine = (lax.axis_size(axis), lax.axis_index(axis))
    pieces = jax.tree.map(lambda part: lax.all_gather(part, axis), value)
    so_far = jax.tree.map(
        lambda part, zero: jnp.full_like(part, 0) + jnp.asarray(zero, part.dtype), value, neutral
    )

    def hop(position, so_far):
        longer = join(so_far, jax.tree.map(lambda part: part[position], pieces))
        return jax.tree.map(lambda new, old: jnp.where(position < mine, new, old), longer, so_far)

    return lax.fori_loop(0, count - 1, hop, so_far)


def join_runs(earlier_run, later_run):
    return (earlier_run[0] * later_run[0], later_run[0] * earlier_run[1] + later_run[1])


def slot_targets(route_block, expert_count, capacity):
    flat_routes = route_block.reshape(-1)
    onehot = (flat_routes[:, None] == jnp.arange(expert_count, dtype=jnp.int32)[None, :]).astype(
        jnp.int32
    )
    earlier_hits = jnp.cumsum(onehot, axis=0) - onehot
    slot_index = jnp.sum(earlier_hits * onehot, axis=1)
    return (flat_routes * capacity + slot_index).reshape(route_block.shape)


def pick_matrix(targets, slot_total):
    slot_hits = targets[None, :, :] == jnp.arange(slot_total, dtype=jnp.int32)[:, None, None]
    return jnp.sum(slot_hits.astype(jnp.int32), axis=2).astype(jnp.bfloat16)


def rms_rows(row_block, gain_vector):
    floated = row_block.astype(jnp.float32)
    inverse_rms = lax.rsqrt(jnp.mean(floated * floated, axis=1, keepdims=True) + EPSILON)
    return (floated * inverse_rms * gain_vector[None, :]).astype(jnp.bfloat16)


def expert_apply(row_piece, gate_weight, up_weight, down_weight):
    gate_part = jnp.dot(row_piece, gate_weight, preferred_element_type=jnp.float32)
    up_part = jnp.dot(row_piece, up_weight, preferred_element_type=jnp.float32)
    hidden_units = (jax.nn.silu(gate_part) * up_part).astype(jnp.bfloat16)
    return jnp.dot(hidden_units, down_weight, preferred_element_type=jnp.float32)


def local_slotted(
    lru_input,
    gate_input,
    documents,
    conv_taps,
    rate_weight,
    inlet_weight,
    decay_param,
    lru_gain,
    out_weight,
    residual,
    ffn_gain,
    routes,
    route_weights,
    w_gate,
    w_up,
    w_down,
):
    positions = lru_input.shape[0]
    channels = lru_input.shape[1]
    model_width = residual.shape[1]
    reach_back = conv_taps.shape[0] - 1
    tail_rows, tail_docs = shifted(
        (lru_input[positions - reach_back :], documents[positions - reach_back :] + 1), "sp", 1
    )
    prior_docs = jnp.concatenate([tail_docs - 1, documents])
    padded_input = jnp.concatenate([tail_rows, lru_input], axis=0)
    conv_sum = jnp.zeros((positions, channels), jnp.float32)
    for tap_index in range(reach_back + 1):
        same_doc = (prior_docs[tap_index : tap_index + positions] == documents).astype(jnp.float32)[
            :, None
        ]
        conv_sum = (
            conv_sum
            + padded_input[tap_index : tap_index + positions].astype(jnp.float32)
            * conv_taps[tap_index].astype(jnp.float32)[None, :]
            * same_doc
        )
    convolved = conv_sum.astype(jnp.bfloat16)
    grouped = convolved.reshape(positions, rate_weight.shape[0], rate_weight.shape[1])
    rate_gate = jax.nn.sigmoid(
        jnp.einsum(
            "tnc,ncd->tnd", grouped, rate_weight, preferred_element_type=jnp.float32
        ).reshape(positions, channels)
    )
    inlet_gate = jax.nn.sigmoid(
        jnp.einsum(
            "tnc,ncd->tnd", grouped, inlet_weight, preferred_element_type=jnp.float32
        ).reshape(positions, channels)
    )
    log_decay = -RATE_SCALE * rate_gate * jax.nn.softplus(-decay_param)[None, :]
    starts = (prior_docs[reach_back - 1 : reach_back - 1 + positions] != documents)[:, None]
    decay_step = jnp.where(starts, 0.0, jnp.exp(log_decay))
    norm_factor = jnp.where(starts, 1.0, jnp.sqrt(-jnp.expm1(2.0 * log_decay)))
    drive_term = norm_factor * inlet_gate * convolved.astype(jnp.float32)
    decay_run, local_state = lax.associative_scan(join_runs, (decay_step, drive_term), axis=0)
    carried = carried_in(
        (decay_run[positions - 1], local_state[positions - 1]),
        "sp",
        join_runs,
        (jnp.ones((channels,), jnp.float32), jnp.zeros((channels,), jnp.float32)),
    )
    hidden_state = local_state + decay_run * carried[1][None, :]
    square_sums = lax.psum(jnp.sum(hidden_state * hidden_state, axis=1), "tp")
    inverse_rms = lax.rsqrt(square_sums[:, None] / (channels * lax.axis_size("tp")) + EPSILON)
    mixer_rows = (
        hidden_state * inverse_rms * lru_gain[None, :] * jax.nn.gelu(gate_input.astype(jnp.float32))
    ).astype(jnp.bfloat16)
    tp_count = lax.axis_size("tp")
    tp_here = lax.axis_index("tp")
    expert_count = lax.axis_size("sp")
    route_rows = positions // tp_count
    top_count = routes.shape[1]
    capacity = 2 * top_count * route_rows // expert_count
    slot_total = expert_count * capacity
    projected = lax.psum_scatter(
        jnp.dot(mixer_rows, out_weight, preferred_element_type=jnp.float32).astype(jnp.bfloat16),
        "tp",
        scatter_dimension=0,
        tiled=True,
    ).astype(jnp.float32)
    own_rows = (
        lax.dynamic_slice_in_dim(residual, tp_here * route_rows, route_rows, 0).astype(jnp.float32)
        + projected
    ).astype(jnp.bfloat16)
    own_routes = lax.dynamic_slice_in_dim(routes, tp_here * route_rows, route_rows, 0)
    targets = slot_targets(own_routes, expert_count, capacity)
    outgoing = jnp.dot(
        pick_matrix(targets, slot_total),
        rms_rows(own_rows, ffn_gain),
        preferred_element_type=jnp.float32,
    ).astype(jnp.bfloat16)
    arrived = lax.all_to_all(
        outgoing.reshape(expert_count, capacity, model_width),
        "sp",
        split_axis=0,
        concat_axis=0,
        tiled=True,
    )
    partial_out = expert_apply(
        lax.all_gather(arrived.reshape(slot_total, model_width), "tp", axis=0, tiled=True),
        w_gate[0],
        w_up[0],
        w_down[0],
    )
    expert_out = lax.psum_scatter(
        partial_out.astype(jnp.bfloat16), "tp", scatter_dimension=0, tiled=True
    )
    returned = lax.all_to_all(
        expert_out.reshape(expert_count, capacity, model_width),
        "sp",
        split_axis=0,
        concat_axis=0,
        tiled=True,
    )
    picked = returned.reshape(slot_total, model_width)[targets.reshape(-1)].astype(jnp.float32)
    picked = picked.reshape(route_rows, top_count, model_width)
    own_weights = lax.dynamic_slice_in_dim(route_weights, tp_here * route_rows, route_rows, 0)
    routed = jnp.sum(picked * own_weights[:, :, None], axis=1)
    return (own_rows.astype(jnp.float32) + routed).astype(jnp.bfloat16)


def local(*arrays):
    positions, top_count = arrays[11].shape
    shards = lax.axis_size("sp")
    route_rows = positions // lax.axis_size("tp")
    dense = shards == PLANE and 2 * top_count * route_rows // shards >= route_rows
    if not dense:
        return local_slotted(*arrays)
    return local_dense(*arrays)


def solution(mesh):
    return jax.shard_map(
        local,
        mesh=mesh,
        in_specs=(
            P("sp", "tp"),
            P("sp", "tp"),
            P("sp"),
            P(None, "tp"),
            P("tp", None, None),
            P("tp", None, None),
            P("tp"),
            P("tp"),
            P("tp", None),
            P("sp", None),
            P(),
            P("sp", None),
            P("sp", None),
            P("sp", None, "tp"),
            P("sp", None, "tp"),
            P("sp", "tp", None),
        ),
        out_specs=P(("sp", "tp"), None),
        check_vma=False,
    )
```

```python
import functools

import jax
import jax.numpy as jnp
from jax import lax
from jax.experimental import pallas as pl
from jax.experimental.pallas import tpu as pltpu
from jax.sharding import PartitionSpec as P


EPSILON = 1e-06
RATE_SCALE = 8.0
LANES = 128
SUBLANES = 8
CORES = 2
PLANE = 4


F32 = jnp.float32
BF16 = jnp.bfloat16


def vmem_call(kernel, outs, args, scratch=(), limit_mib=4, far_args=()):
    near, far = (pl.BlockSpec(memory_space=space) for space in (pltpu.VMEM, pltpu.HBM))
    return pl.pallas_call(
        kernel,
        in_specs=[far] * len(far_args) + [near] * len(args),
        out_specs=[near] * len(outs),
        out_shape=[jax.ShapeDtypeStruct(shape, dtype) for shape, dtype in outs],
        scratch_shapes=[
            pltpu.VMEM(*what) if isinstance(what, tuple) else what for what in scratch
        ],
        compiler_params=pltpu.CompilerParams(vmem_limit_bytes=limit_mib << 20),
    )(
        *[pltpu.with_memory_space_constraint(arg, pltpu.HBM) for arg in far_args],
        *[pltpu.with_memory_space_constraint(arg, pltpu.VMEM) for arg in args],
    )


def place():
    tp_here = lax.axis_index("tp")
    return lax.axis_index("sp"), tp_here // CORES, tp_here % CORES


def flip(value, axis, distance):
    return lax.ppermute(value, axis, [(i, i ^ distance) for i in range(lax.axis_size(axis))])


def flip_plane(value, order):
    tp_count = lax.axis_size("tp")
    pairs = [
        (shard * tp_count + at, (shard ^ plane_flip(at % CORES, order)) * tp_count + at)
        for shard in range(PLANE)
        for at in range(tp_count)
    ]
    return lax.ppermute(value, ("sp", "tp"), pairs)


def plane_flip(core, order):
    return 1 + core if order == 0 else 2 - core


def flip_z(value, distance):
    return flip(value, "tp", distance * CORES)


def column(row):
    return jnp.transpose(jnp.broadcast_to(row, (LANES, row.shape[1])))


def one_minus_exp(value):
    series = jnp.ones_like(value)
    for order in range(7, 1, -1):
        series = 1.0 + value * series * (1.0 / order)
    return jnp.where(value > -0.35, -value * series, 1.0 - jnp.exp(value))


def scan_rows(decay, drive):
    rows = decay.shape[0]
    row_ids = lax.broadcasted_iota(jnp.int32, decay.shape, 0)
    distance = 1
    while distance < rows:
        if distance < SUBLANES:
            head = row_ids < distance
            earlier_decay = jnp.where(head, 1.0, pltpu.roll(decay, distance, 0))
            earlier_drive = jnp.where(head, 0.0, pltpu.roll(drive, distance, 0))
            drive = drive + decay * earlier_drive
            decay = decay * earlier_decay
        else:
            late_drive = drive[distance:] + decay[distance:] * drive[: rows - distance]
            late_decay = decay[distance:] * decay[: rows - distance]
            drive = jnp.concatenate([drive[:distance], late_drive], axis=0)
            decay = jnp.concatenate([decay[:distance], late_decay], axis=0)
        distance *= 2
    return decay, drive


def gated_terms(conv, starts, rate_w, inlet_w, decay_in):
    conv = conv.astype(BF16)
    rate = jax.nn.sigmoid(jnp.dot(conv, rate_w, preferred_element_type=F32))
    inlet = jax.nn.sigmoid(jnp.dot(conv, inlet_w, preferred_element_type=F32))
    negated = -decay_in
    soft = jnp.maximum(negated, 0.0) + jnp.log1p(jnp.exp(-jnp.abs(negated)))
    log_decay = -RATE_SCALE * rate * soft
    decay = jnp.where(starts, 0.0, jnp.exp(log_decay))
    norm = jnp.where(starts, 1.0, jnp.sqrt(one_minus_exp(2.0 * log_decay)))
    return decay, norm * inlet * conv.astype(F32)


def convolve(padded, docs, taps, at, count, lanes):
    reach = taps.shape[0] - 1
    own_doc = docs[at : at + count]
    conv = jnp.zeros((count, LANES), F32)
    for tap in range(reach + 1):
        source = slice(at - reach + tap, at - reach + tap + count)
        rows = padded[source, lanes]
        if tap < reach:
            rows = jnp.where(docs[source] == own_doc, rows, 0.0)
        conv = conv + rows * taps[tap : tap + 1, lanes].astype(F32)
    return conv, docs[at - 1 : at - 1 + count] != own_doc


EDGE = slice(SUBLANES, 2 * SUBLANES)
EDGE_DOCS = slice(2 * SUBLANES, 3 * SUBLANES)
MESSAGE_ROWS = 3 * SUBLANES


def lru_kernel(*refs):
    far, refs = refs[:12], refs[12:]
    (state_out, run_out, mix_out), refs = refs[:3], refs[3:]
    messages, refs = refs[:PLANE], refs[PLANE:]
    (taps, rate_w, inlet_w, decay_in, out_w, residual), refs = refs[:6], refs[6:]
    rows_in, gate_in, docs, gain, routes, route_w, padded, doc_cols, sems = refs
    block = residual.shape[0]
    own = pl.ds(pl.multiple_of(lax.axis_index("tp") * block, block), block)
    sources = [*far[:11], far[11].at[own]]
    targets = (
        rows_in, docs, taps, rate_w, inlet_w, decay_in, gate_in, gain, routes, route_w, out_w, residual,
    )
    copies = [
        pltpu.make_async_copy(source, target, sems.at[i])
        for i, (source, target) in enumerate(zip(sources, targets))
    ]
    for copy in copies:
        copy.start()
    for copy in copies[:-2]:
        copy.wait()
    positions, channels = rows_in.shape
    reach = taps.shape[0] - 1
    padded[0:SUBLANES] = jnp.zeros((SUBLANES, channels), F32)
    padded[SUBLANES:] = rows_in[...].astype(F32)
    doc_cols[0:SUBLANES] = jnp.zeros((SUBLANES, LANES), F32)
    doc_cols[SUBLANES:] = column(docs[...].astype(F32) + 1.0)
    later = lax.broadcasted_iota(jnp.int32, (positions, LANES), 0) >= reach
    for group in range(channels // LANES):
        lanes = slice(group * LANES, (group + 1) * LANES)
        conv, starts = convolve(padded, doc_cols, taps, SUBLANES, positions, lanes)
        decay, drive = gated_terms(
            conv, starts, rate_w[group], inlet_w[group], decay_in[0:1, lanes]
        )
        run, state = scan_rows(jnp.where(later, decay, 1.0), jnp.where(later, drive, 0.0))
        state_out[:, lanes] = state
        run_out[:, lanes] = run
        for message in messages:
            message[0:1, lanes] = run[positions - 1 :]
            message[1:2, lanes] = state[positions - 1 :]
        mix_out[:, lanes] = jax.nn.gelu(gate_in[:, lanes].astype(F32)) * gain[0:1, lanes]

    def ends(rows):
        begin, end = rows[SUBLANES : 2 * SUBLANES], rows[positions : positions + SUBLANES]
        row_ids = lax.broadcasted_iota(jnp.int32, begin.shape, 0)
        return jnp.where(row_ids < reach, begin, end)

    shard, _, _ = place()
    for k, message in enumerate(messages):
        dense = jnp.zeros((1, positions), F32)
        for choice in range(routes.shape[0]):
            chosen = routes[choice : choice + 1] == (shard ^ k)
            dense = dense + jnp.where(chosen, route_w[choice : choice + 1], 0.0)
        message[2:3, 0:positions] = dense
        message[EDGE, 0:channels] = ends(padded)
        message[EDGE_DOCS, 0:LANES] = ends(doc_cols)
    for copy in copies[-2:]:
        copy.wait()


def fetch_kernel(far, near, sems):
    count = sems.shape[0]
    rows = far.shape[0] // count
    pieces = [pl.ds(i * rows, rows) for i in range(count)]
    copies = [
        pltpu.make_async_copy(far.at[piece], near.at[piece], sems.at[i])
        for i, piece in enumerate(pieces)
    ]
    for copy in copies:
        copy.start()
    for copy in copies:
        copy.wait()


def split_sum(total):
    lane_ids = lax.broadcasted_iota(jnp.int32, (total.shape[0], LANES), 1)
    high = total.astype(BF16).astype(F32)
    low = (total - high).astype(BF16).astype(F32)
    return jnp.where(lane_ids == 0, high, jnp.where(lane_ids == 1, low, 0.0)).astype(BF16)


def joined_sum(lanes):
    lanes = lanes.astype(F32)
    return lanes[:, 0:1] + lanes[:, 1:2]


def mix_kernel(state, run, mix, taps, rate_w, inlet_w, decay_in, *rest, block):
    *messages, keep, send, stacked, edge, edge_docs, terms, heads, hidden, mixed = rest
    channels = state.shape[1]
    reach = taps.shape[0] - 1
    for k, message in enumerate(messages):
        stacked[k] = message[...]
    shard, _, core = place()
    pair = 2 * SUBLANES
    for j in range(PLANE):
        here = stacked.at[j ^ shard]
        at = j * pair
        if j == 0:
            edge[at : at + SUBLANES] = jnp.zeros((SUBLANES, channels), F32)
            edge_docs[at : at + SUBLANES] = jnp.zeros((SUBLANES, LANES), F32)
        else:
            before = stacked.at[(j - 1) ^ shard]
            edge[at : at + SUBLANES] = before[EDGE, :channels]
            edge_docs[at : at + SUBLANES] = before[EDGE_DOCS, :LANES]
        edge[at + SUBLANES : at + pair] = here[EDGE, :channels]
        edge_docs[at + SUBLANES : at + pair] = here[EDGE_DOCS, :LANES]
    for group in range(channels // LANES):
        lanes = slice(group * LANES, (group + 1) * LANES)
        firsts = [
            convolve(edge, edge_docs, taps, j * pair + SUBLANES, SUBLANES, lanes)
            for j in range(PLANE)
        ]
        conv = jnp.concatenate([first[0] for first in firsts], axis=0)
        for j, (_, starts) in enumerate(firsts):
            rows = slice(j * SUBLANES, (j + 1) * SUBLANES)
            heads[j, :, lanes] = jnp.where(starts, 1.0, 0.0)
        starts = jnp.concatenate([heads[j, :, lanes] for j in range(PLANE)], axis=0) > 0.5
        terms[0, :, lanes], terms[1, :, lanes] = gated_terms(
            conv, starts, rate_w[group], inlet_w[group], decay_in[0:1, lanes]
        )
    carried = jnp.zeros((1, channels), F32)
    for j in range(PLANE):
        for row in range(reach):
            at = j * SUBLANES + row
            carried = terms[0, at : at + 1] * carried + terms[1, at : at + 1]
            heads[j, row : row + 1] = carried
        here = stacked.at[j ^ shard]
        carried = here[0:1, :channels] * carried + here[1:2, :channels]
    head = heads[shard]
    hidden[...] = state[...] + run[...] * head[reach - 1 : reach]
    early = lax.broadcasted_iota(jnp.int32, (SUBLANES, channels), 0) < reach
    hidden[0:SUBLANES] = jnp.where(early, head, hidden[0:SUBLANES])
    whole = hidden[...]
    mixed[:, :channels] = (whole * mix[...]).astype(BF16)
    mixed[:, channels:] = split_sum(jnp.sum(whole * whole, axis=1, keepdims=True))
    for z in range(keep.shape[0] // block):
        rows = slice(z * block, (z + 1) * block)
        keep[rows] = mixed[pl.ds(pl.multiple_of((CORES * z + core) * block, block), block)]
        send[rows] = mixed[pl.ds(pl.multiple_of((CORES * z + 1 - core) * block, block), block)]


def project_kernel(keep, other, own_w, other_w, *rest, block):
    *outs, own_rows, other_rows = rest
    channels, width = own_w.shape
    _, depth, _ = place()
    for k in range(len(outs)):
        rows = slice(k * block, (k + 1) * block)
        source = pl.ds(pl.multiple_of((depth ^ k) * block, block), block)
        own_rows[rows] = keep[source]
        other_rows[rows] = other[source]
    squares = split_sum(joined_sum(own_rows[:, channels:]) + joined_sum(other_rows[:, channels:]))
    product = jnp.dot(own_rows[:, :channels], own_w[...], preferred_element_type=F32)
    product = product + jnp.dot(other_rows[:, :channels], other_w[...], preferred_element_type=F32)
    for k, out in enumerate(outs):
        rows = slice(k * block, (k + 1) * block)
        out[:, :width] = product[rows].astype(BF16)
        out[:, width:] = squares[rows]


def add_kernel(one, two, out):
    width = out.shape[1] - LANES
    out[:, :width] = (one[:, :width].astype(F32) + two[:, :width].astype(F32)).astype(BF16)
    out[:, width:] = split_sum(joined_sum(one[:, width:]) + joined_sum(two[:, width:]))


def norm_kernel(residual, gain, *rest, channels_total):
    *parts, after_out, normed_out = rest
    width = residual.shape[1]
    total = sum(part[:, :width].astype(F32) for part in parts)
    squares = sum(joined_sum(part[:, width:]) for part in parts)
    projected = total * lax.rsqrt(squares / channels_total + EPSILON)
    after = (residual[...].astype(F32) + projected).astype(BF16)
    after_out[...] = after
    floated = after.astype(F32)
    inverse_rms = lax.rsqrt(jnp.mean(floated * floated, axis=1, keepdims=True) + EPSILON)
    normed_out[...] = (floated * inverse_rms * gain[...]).astype(BF16)


def expert_kernel(*refs, z_flips, block, tile, out_tile):
    pieces, refs = refs[:2], refs[2:]
    messages, refs = refs[:PLANE], refs[PLANE:]
    (own_gate, other_gate, own_up, other_up, own_down, other_down), refs = refs[:6], refs[6:]
    outs, (tokens, weight_cols, weights, hidden) = refs[:2], refs[2:]
    half, width = own_down.shape
    positions = weight_cols.shape[1]
    _, depth, core = place()
    for k in range(PLANE):
        weight_cols[k] = column(messages[k][2:3, :positions])
    planes = ((0, plane_flip(core, 0)), (plane_flip(core, 1), PLANE - 1))
    at = 0
    for piece, halves in zip(pieces, planes):
        tokens[at : at + piece.shape[0]] = piece[...]
        for k in halves:
            for z_flip in z_flips:
                source = pl.multiple_of((CORES * (depth ^ z_flip) + core) * block, block)
                weights[at : at + block] = weight_cols[k, pl.ds(source, block)]
                at += block

    for base, gate_w, up_w in ((0, own_gate, own_up), (half, other_gate, other_up)):

        def hide(index, _):
            spot = pl.multiple_of(index * tile, LANES)
            gate = jnp.dot(tokens[...], gate_w[:, pl.ds(spot, tile)], preferred_element_type=F32)
            up = jnp.dot(tokens[...], up_w[:, pl.ds(spot, tile)], preferred_element_type=F32)
            spot = pl.multiple_of(base + spot, LANES)
            hidden[:, pl.ds(spot, tile)] = (jax.nn.silu(gate) * up).astype(BF16)
            return _

        lax.fori_loop(0, half // tile, hide, 0)

    def lower(index, _):
        cols = pl.ds(pl.multiple_of(index * out_tile, LANES), out_tile)
        product = jnp.dot(hidden[:, :half], own_down[:, cols], preferred_element_type=F32)
        product = product + jnp.dot(hidden[:, half:], other_down[:, cols], preferred_element_type=F32)
        scale = jnp.concatenate([weights[...]] * (out_tile // LANES), axis=1)
        scaled = (product * scale).astype(BF16)
        at = 0
        for out in outs:
            out[:, cols] = scaled[at : at + out.shape[0]]
            at += out.shape[0]
        return _

    lax.fori_loop(0, width // out_tile, lower, 0)


def run_experts(pieces, z_flips, messages, weights, block):
    half, width = weights[-1].shape
    rows = sum(piece.shape[0] for piece in pieces)
    positions = block * lax.axis_size("tp")
    return vmem_call(
        functools.partial(
            expert_kernel, z_flips=z_flips, block=block, tile=half, out_tile=width // 2
        ),
        [(piece.shape, BF16) for piece in pieces],
        [*pieces, *messages, *weights],
        scratch=[
            ((rows, width), BF16),
            ((PLANE, positions, LANES), F32),
            ((rows, LANES), F32),
            ((rows, 2 * half), BF16),
        ],
        limit_mib=10,
    )


def float_sum(parts):
    return sum(part.astype(F32) for part in parts)


def spread(rows):
    near = flip_plane(rows, 0)
    pair = jnp.concatenate([rows, near])
    return [pair, flip_plane(pair, 1)]


def gather_sum(outs):
    half = outs[0].shape[0] // 2
    far = flip_plane(outs[1], 1)
    near = float_sum([outs[0][half:], far[half:]]).astype(BF16)
    near = flip_plane(near, 0)
    return float_sum([outs[0][:half], far[:half], near]).astype(BF16)


def local_dense(
    lru_input, gate_input, documents, conv_taps, rate_weight, inlet_weight, decay_param, lru_gain,
    out_weight, residual, ffn_gain, routes, route_weights, w_gate, w_up, w_down,
):
    positions, channels = lru_input.shape
    width = residual.shape[1]
    tp_count = lax.axis_size("tp")
    depths = tp_count // CORES
    block = positions // tp_count
    span = max(positions, channels)

    other_out = flip(out_weight, "tp", 1)

    state, run, mix, *rest = vmem_call(
        lru_kernel,
        [((positions, channels), F32)] * 3
        + [((MESSAGE_ROWS, span), F32)] * PLANE
        + [
            (conv_taps.shape, BF16), (rate_weight.shape, BF16), (inlet_weight.shape, BF16),
            ((1, channels), F32), (out_weight.shape, BF16), ((block, width), BF16),
        ],
        [],
        scratch=[
            ((positions, channels), BF16),
            ((positions, channels), BF16),
            ((1, positions), jnp.int32),
            ((1, channels), F32),
            (routes.T.shape, jnp.int32),
            (routes.T.shape, F32),
            ((SUBLANES + positions, channels), F32),
            ((SUBLANES + positions, LANES), F32),
            pltpu.SemaphoreType.DMA((12,)),
        ],
        far_args=[
            lru_input, documents[None, :], conv_taps, rate_weight, inlet_weight,
            decay_param[None, :], gate_input, lru_gain[None, :], routes.T, route_weights.T,
            out_weight, residual,
        ],
    )
    messages, params = rest[:PLANE], rest[PLANE:]
    taps, rate_w, inlet_w, decay_in, own_out, own_residual = params
    messages = [messages[0]] + [flip(messages[k], "sp", k) for k in range(1, PLANE)]
    messages, other_out = lax.optimization_barrier((messages, other_out))

    half_rows = positions // CORES
    packed = (half_rows, channels + LANES)
    keep, send = vmem_call(
        functools.partial(mix_kernel, block=block),
        [(packed, BF16)] * 2,
        [state, run, mix, taps, rate_w, inlet_w, decay_in, *messages],
        scratch=[
            ((PLANE, MESSAGE_ROWS, span), F32),
            ((2 * PLANE * SUBLANES, channels), F32),
            ((2 * PLANE * SUBLANES, LANES), F32),
            ((2, PLANE * SUBLANES, channels), F32),
            ((PLANE, SUBLANES, channels), F32),
            ((positions, channels), F32),
            ((positions, channels + LANES), BF16),
        ],
    )
    other, *own = lax.optimization_barrier((flip(send, "tp", 1), w_gate[0], w_up[0], w_down[0]))
    swapped = [flip(value, "tp", 1) for value in own]
    parts = vmem_call(
        functools.partial(project_kernel, block=block),
        [((block, width + LANES), BF16)] * depths,
        [keep, other, own_out, other_out],
        scratch=[(packed, BF16)] * 2,
    )
    [own_down] = vmem_call(
        fetch_kernel,
        [(w_down.shape[1:], BF16)],
        [],
        scratch=[pltpu.SemaphoreType.DMA((4,))],
        far_args=[w_down[0]],
    )
    parts = dict(enumerate(parts))
    for k in range(depths - 1, 1, -1):
        relay = k & -k
        if relay != k:
            passed = flip_z(parts.pop(k), relay)
            [parts[k ^ relay]] = vmem_call(
                add_kernel, [((block, width + LANES), BF16)], [parts[k ^ relay], passed]
            )
    parts = [parts[k] if k == 0 else flip_z(parts[k], k) for k in parts]
    after, normed = vmem_call(
        functools.partial(norm_kernel, channels_total=channels * tp_count),
        [((block, width), BF16)] * 2,
        [own_residual, ffn_gain[None, :], *parts],
    )

    weights = (w_gate[0], swapped[0], w_up[0], swapped[1], own_down, swapped[2])
    rows_at = [normed] + [flip_z(normed, k) for k in range(1, depths)]
    total = after.astype(F32)
    for k in range(depths):
        pieces = spread(rows_at[k])
        outs = run_experts(pieces, (k,), messages, weights, block)
        summed = gather_sum(outs)
        total = total + (flip_z(summed, k) if k else summed).astype(F32)
    return total.astype(BF16)


def shifted(block, axis, distance):
    devices = range(lax.axis_size(axis))
    route = [(i - distance, i) for i in devices if i - distance in devices]
    return lax.ppermute(block, axis, route)


def carried_in(value, axis, join, neutral):
    count, mine = (lax.axis_size(axis), lax.axis_index(axis))
    pieces = jax.tree.map(lambda part: lax.all_gather(part, axis), value)
    so_far = jax.tree.map(
        lambda part, zero: jnp.full_like(part, 0) + jnp.asarray(zero, part.dtype), value, neutral
    )

    def hop(position, so_far):
        longer = join(so_far, jax.tree.map(lambda part: part[position], pieces))
        return jax.tree.map(lambda new, old: jnp.where(position < mine, new, old), longer, so_far)

    return lax.fori_loop(0, count - 1, hop, so_far)


def join_runs(earlier_run, later_run):
    return (earlier_run[0] * later_run[0], later_run[0] * earlier_run[1] + later_run[1])


def slot_targets(route_block, expert_count, capacity):
    flat_routes = route_block.reshape(-1)
    onehot = (flat_routes[:, None] == jnp.arange(expert_count, dtype=jnp.int32)[None, :]).astype(
        jnp.int32
    )
    earlier_hits = jnp.cumsum(onehot, axis=0) - onehot
    slot_index = jnp.sum(earlier_hits * onehot, axis=1)
    return (flat_routes * capacity + slot_index).reshape(route_block.shape)


def pick_matrix(targets, slot_total):
    slot_hits = targets[None, :, :] == jnp.arange(slot_total, dtype=jnp.int32)[:, None, None]
    return jnp.sum(slot_hits.astype(jnp.int32), axis=2).astype(jnp.bfloat16)


def rms_rows(row_block, gain_vector):
    floated = row_block.astype(jnp.float32)
    inverse_rms = lax.rsqrt(jnp.mean(floated * floated, axis=1, keepdims=True) + EPSILON)
    return (floated * inverse_rms * gain_vector[None, :]).astype(jnp.bfloat16)


def expert_apply(row_piece, gate_weight, up_weight, down_weight):
    gate_part = jnp.dot(row_piece, gate_weight, preferred_element_type=jnp.float32)
    up_part = jnp.dot(row_piece, up_weight, preferred_element_type=jnp.float32)
    hidden_units = (jax.nn.silu(gate_part) * up_part).astype(jnp.bfloat16)
    return jnp.dot(hidden_units, down_weight, preferred_element_type=jnp.float32)


def local_slotted(
    lru_input,
    gate_input,
    documents,
    conv_taps,
    rate_weight,
    inlet_weight,
    decay_param,
    lru_gain,
    out_weight,
    residual,
    ffn_gain,
    routes,
    route_weights,
    w_gate,
    w_up,
    w_down,
):
    positions = lru_input.shape[0]
    channels = lru_input.shape[1]
    model_width = residual.shape[1]
    reach_back = conv_taps.shape[0] - 1
    tail_rows, tail_docs = shifted(
        (lru_input[positions - reach_back :], documents[positions - reach_back :] + 1), "sp", 1
    )
    prior_docs = jnp.concatenate([tail_docs - 1, documents])
    padded_input = jnp.concatenate([tail_rows, lru_input], axis=0)
    conv_sum = jnp.zeros((positions, channels), jnp.float32)
    for tap_index in range(reach_back + 1):
        same_doc = (prior_docs[tap_index : tap_index + positions] == documents).astype(jnp.float32)[
            :, None
        ]
        conv_sum = (
            conv_sum
            + padded_input[tap_index : tap_index + positions].astype(jnp.float32)
            * conv_taps[tap_index].astype(jnp.float32)[None, :]
            * same_doc
        )
    convolved = conv_sum.astype(jnp.bfloat16)
    grouped = convolved.reshape(positions, rate_weight.shape[0], rate_weight.shape[1])
    rate_gate = jax.nn.sigmoid(
        jnp.einsum(
            "tnc,ncd->tnd", grouped, rate_weight, preferred_element_type=jnp.float32
        ).reshape(positions, channels)
    )
    inlet_gate = jax.nn.sigmoid(
        jnp.einsum(
            "tnc,ncd->tnd", grouped, inlet_weight, preferred_element_type=jnp.float32
        ).reshape(positions, channels)
    )
    log_decay = -RATE_SCALE * rate_gate * jax.nn.softplus(-decay_param)[None, :]
    starts = (prior_docs[reach_back - 1 : reach_back - 1 + positions] != documents)[:, None]
    decay_step = jnp.where(starts, 0.0, jnp.exp(log_decay))
    norm_factor = jnp.where(starts, 1.0, jnp.sqrt(-jnp.expm1(2.0 * log_decay)))
    drive_term = norm_factor * inlet_gate * convolved.astype(jnp.float32)
    decay_run, local_state = lax.associative_scan(join_runs, (decay_step, drive_term), axis=0)
    carried = carried_in(
        (decay_run[positions - 1], local_state[positions - 1]),
        "sp",
        join_runs,
        (jnp.ones((channels,), jnp.float32), jnp.zeros((channels,), jnp.float32)),
    )
    hidden_state = local_state + decay_run * carried[1][None, :]
    square_sums = lax.psum(jnp.sum(hidden_state * hidden_state, axis=1), "tp")
    inverse_rms = lax.rsqrt(square_sums[:, None] / (channels * lax.axis_size("tp")) + EPSILON)
    mixer_rows = (
        hidden_state * inverse_rms * lru_gain[None, :] * jax.nn.gelu(gate_input.astype(jnp.float32))
    ).astype(jnp.bfloat16)
    tp_count = lax.axis_size("tp")
    tp_here = lax.axis_index("tp")
    expert_count = lax.axis_size("sp")
    route_rows = positions // tp_count
    top_count = routes.shape[1]
    capacity = 2 * top_count * route_rows // expert_count
    slot_total = expert_count * capacity
    projected = lax.psum_scatter(
        jnp.dot(mixer_rows, out_weight, preferred_element_type=jnp.float32).astype(jnp.bfloat16),
        "tp",
        scatter_dimension=0,
        tiled=True,
    ).astype(jnp.float32)
    own_rows = (
        lax.dynamic_slice_in_dim(residual, tp_here * route_rows, route_rows, 0).astype(jnp.float32)
        + projected
    ).astype(jnp.bfloat16)
    own_routes = lax.dynamic_slice_in_dim(routes, tp_here * route_rows, route_rows, 0)
    targets = slot_targets(own_routes, expert_count, capacity)
    outgoing = jnp.dot(
        pick_matrix(targets, slot_total),
        rms_rows(own_rows, ffn_gain),
        preferred_element_type=jnp.float32,
    ).astype(jnp.bfloat16)
    arrived = lax.all_to_all(
        outgoing.reshape(expert_count, capacity, model_width),
        "sp",
        split_axis=0,
        concat_axis=0,
        tiled=True,
    )
    partial_out = expert_apply(
        lax.all_gather(arrived.reshape(slot_total, model_width), "tp", axis=0, tiled=True),
        w_gate[0],
        w_up[0],
        w_down[0],
    )
    expert_out = lax.psum_scatter(
        partial_out.astype(jnp.bfloat16), "tp", scatter_dimension=0, tiled=True
    )
    returned = lax.all_to_all(
        expert_out.reshape(expert_count, capacity, model_width),
        "sp",
        split_axis=0,
        concat_axis=0,
        tiled=True,
    )
    picked = returned.reshape(slot_total, model_width)[targets.reshape(-1)].astype(jnp.float32)
    picked = picked.reshape(route_rows, top_count, model_width)
    own_weights = lax.dynamic_slice_in_dim(route_weights, tp_here * route_rows, route_rows, 0)
    routed = jnp.sum(picked * own_weights[:, :, None], axis=1)
    return (own_rows.astype(jnp.float32) + routed).astype(jnp.bfloat16)


def local(*arrays):
    positions, top_count = arrays[11].shape
    shards = lax.axis_size("sp")
    route_rows = positions // lax.axis_size("tp")
    dense = shards == PLANE and 2 * top_count * route_rows // shards >= route_rows
    if not dense:
        return local_slotted(*arrays)
    return local_dense(*arrays)


def solution(mesh):
    return jax.shard_map(
        local,
        mesh=mesh,
        in_specs=(
            P("sp", "tp"),
            P("sp", "tp"),
            P("sp"),
            P(None, "tp"),
            P("tp", None, None),
            P("tp", None, None),
            P("tp"),
            P("tp"),
            P("tp", None),
            P("sp", None),
            P(),
            P("sp", None),
            P("sp", None),
            P("sp", None, "tp"),
            P("sp", None, "tp"),
            P("sp", "tp", None),
        ),
        out_specs=P(("sp", "tp"), None),
        check_vma=False,
    )
```
